256 devices in a mesh: kv: 32 (over z, y), tp: 8 (over x, core).
Axes of the slice: x: 4, y: 4, z: 8, core: 2. Of those that a mesh axis runs over, the one named last changes fastest.
Arguments:
- tokens: bfloat16 [128, 4096], P(None, 'kv'), may hold values from -8 to 8, as said below
- attn_gain: float32 [4096], P('kv'), may hold values from 0.1 to 1.9
- query_weight: bfloat16 [4096, 1024], P('kv', 'tp'), may hold values from -0.09375 to 0.09375
- key_weight: bfloat16 [4096, 1024], P('kv', 'tp'), may hold values from -0.09375 to 0.09375
- value_weight: bfloat16 [4096, 2048], P('kv', 'tp'), may hold values from -0.09375 to 0.09375
- outgate_weight: bfloat16 [4096, 2048], P('kv', 'tp'), may hold values from -0.09375 to 0.09375
- code_weight: bfloat16 [4096, 16], P('kv'), may hold values from -0.09375 to 0.09375
- decay_weight: bfloat16 [16, 1024], P(None, 'tp'), may hold values from -6 to 6
- decay_bias: float32 [1024], P('tp'), may hold values from -4 to 2
- head_gain: float32 [256], replicated, may hold values from 0.1 to 1.9
- key_cache: bfloat16 [128, 64, 8, 128], P('kv', None, 'tp'), may hold values from -6 to 6
- value_cache: bfloat16 [128, 64, 8, 256], P('kv', None, 'tp'), may hold values from -6 to 6
- decay_cache: float32 [128, 64, 8, 128], P('kv', None, 'tp'), may hold values from -1.1 to 0
- carried_state: float32 [128, 8, 128, 256], P('kv', 'tp'), may hold values from -24 to 24
- lengths: int32 [128], P('kv'), may hold values from 1 to 64, 3328 in all
- output_weight: bfloat16 [2048, 4096], P('tp', 'kv'), may hold values from -0.125 to 0.125
- mlp_gain: float32 [4096], P('kv'), may hold values from 0.1 to 1.9
- gate_weight: bfloat16 [4096, 11008], P('kv', 'tp'), may hold values from -0.09375 to 0.09375
- up_weight: bfloat16 [4096, 11008], P('kv', 'tp'), may hold values from -0.09375 to 0.09375
- down_weight: bfloat16 [11008, 4096], P('tp', 'kv'), may hold values from -0.0546875 to 0.0546875
Outputs:
- layer_out: bfloat16 [128, 4096], P(None, 'kv')
- new_keys: bfloat16 [128, 8, 128], P('kv', 'tp')
- new_values: bfloat16 [128, 8, 256], P('kv', 'tp')
The draws below stay inside these ranges and needn't reach their ends.
Inputs may be any that keep to these rules, and one draw needn't show every extreme that they name: `tokens`: the features of a row have unlike scales. Sequence b's new token comes right after its lengths[b] live positions; positions from lengths[b] on take no part.
All inputs are finite; a program needn't handle non-finite values. No bound on the sum of `lengths` on one device may be relied on, other than what follows from the above.
Results may differ from the reference program's by a relative error of at most 0.025.
Values may be sent and summed in bfloat16 or wider, within the bound.
No kernel may reach another device: no remote copies, remote signals or barrier semaphores. Data moves between devices by JAX's collectives and lax.ppermute only.
A program may use at most 64 MiB of HBM per device.

```python
import math
import jax
import jax.numpy as jnp
import numpy as np
from jax import lax

WIDTH = 4096
HEAD_COUNT = 8
KEY_DIM = 128
VALUE_DIM = 256
KEY_WIDTH = 1024
VALUE_WIDTH = 2048
GATE_RANK = 16
MLP_WIDTH = 11008
BLOCK_SPAN = 64
BATCH_TOTAL = 128
N_TP = 8


def draw_tokens(key, part):
    base_key, rough_key = jax.random.split(jax.random.fold_in(key, 11), 2)
    column = jnp.arange(WIDTH, dtype=jnp.float32) / WIDTH
    jaggedness = jax.random.uniform(rough_key, (WIDTH,), jnp.float32, 0.5, 2.0)
    scales = 10.0 ** (column - 0.75) * jaggedness
    values = jax.random.normal(base_key, (BATCH_TOTAL, WIDTH), jnp.float32) * scales[None, :]
    return jnp.clip(values, -8.0, 8.0).astype(jnp.bfloat16)


def draw_decay_cache(key, part):
    random_split_keys = jax.random.split(jax.random.fold_in(key, 23), 5)
    slowest = 0.002
    fastest = 0.12
    channel_frequencies = jnp.exp(jax.random.uniform(random_split_keys[0], (1, 1, HEAD_COUNT, KEY_DIM), jnp.float32, math.log(slowest), math.log(fastest)))
    sequence_wise = jnp.exp(jax.random.uniform(random_split_keys[1], (BATCH_TOTAL, 1, 1, 1), jnp.float32, math.log(0.5), math.log(2.0)))
    jaggedness = jax.random.uniform(random_split_keys[2], (BATCH_TOTAL, BLOCK_SPAN, HEAD_COUNT, KEY_DIM), jnp.float32, 0.5, 1.5)
    spike_events = jax.random.randint(random_split_keys[3], (BATCH_TOTAL, BLOCK_SPAN, 1, 1), 0, BLOCK_SPAN) < 3
    spike_removal = jax.random.uniform(random_split_keys[4], (BATCH_TOTAL, BLOCK_SPAN, HEAD_COUNT, 1), jnp.float32, math.log(0.5), math.log(0.8))
    return -channel_frequencies * sequence_wise * jaggedness + jnp.where(spike_events, spike_removal, 0.0)


def levels(stream_key, extent, shards, smallest, top_value):
    def one(dim, blocks):
        heights = jax.random.uniform(jax.random.fold_in(jax.random.fold_in(stream_key, 6), dim), (blocks,), jnp.float32, smallest / len(shards), top_value / len(shards))
        return jnp.repeat(jnp.exp(heights), extent[dim] // blocks).reshape((-1,) + (1,) * (len(extent) - dim - 1))

    level = one(*shards[0])
    for cut in shards[1:]:
        level = level * one(*cut)
    return level


def split_up(amount, total, limit, slope):
    loads = [(1 << 20) // math.isqrt(grade ** slope) + 1 for grade in range(2, amount + 1)]
    surplus, given = total - limit - (amount - 1), [1] * (amount - 1)
    while surplus > 0:
        candidates = [i for i in range(amount - 1) if given[i] < limit]
        whole, remaining = sum([loads[i] for i in candidates]), surplus
        for i in candidates:
            more = min(limit - given[i], max(1, remaining * loads[i] // whole), surplus)
            given[i] = given[i] + more
            surplus = surplus - more
    return np.array([limit] + given)


def ragged_sizes(own_key, count, total, limit, slope):
    if count == 2:
        one = jax.random.randint(own_key, (), max(1, total - limit), min(limit, total - 1) + 1)
        return jnp.stack([one, total - one])
    sizes = jnp.asarray(split_up(count, total, limit, slope), jnp.int32)
    couples = (count - 1) // 2
    source_of, taker = sizes[1:1 + 2 * couples:2], sizes[2:2 + 2 * couples:2]
    room = jnp.minimum(source_of - 1, limit - taker)
    shifted = jax.random.randint(jax.random.fold_in(own_key, 1), (couples,), 0, 1 << 20) % (room + 1)
    sizes = sizes.at[1:1 + 2 * couples:2].set(source_of - shifted).at[2:2 + 2 * couples:2].set(taker + shifted)
    return sizes[jax.random.permutation(jax.random.fold_in(own_key, 2), count)]


def scatter_about(own_key, dims, scale, most, pieces=(), kind=jnp.bfloat16):
    result = jax.random.normal(own_key, dims, jnp.float32) * scale
    if len(pieces) > 0:
        result = levels(own_key, dims, pieces, -0.22, 0.18) * result
    return jnp.clip(result, min=-most, max=most).astype(kind)


def setup_inputs(seed: int = 0) -> dict:
    streams_of = jax.random.split(jax.random.key(seed), 21)
    return {
        "tokens": draw_tokens(jax.random.fold_in(streams_of[20], 71), 0),
        "attn_gain": jnp.clip(1.0 + 0.18 * jax.random.normal(streams_of[1], (WIDTH,), jnp.float32), 0.1, 1.9),
        "query_weight": scatter_about(streams_of[2], (WIDTH, KEY_WIDTH), WIDTH ** -0.5, 0.09375, ((0, 32), (1, 8))),
        "key_weight": scatter_about(streams_of[3], (WIDTH, KEY_WIDTH), WIDTH ** -0.5, 0.09375, ((0, 32), (1, 8))),
        "value_weight": scatter_about(streams_of[4], (WIDTH, VALUE_WIDTH), WIDTH ** -0.5, 0.09375, ((0, 32), (1, 8))),
        "outgate_weight": scatter_about(streams_of[5], (WIDTH, VALUE_WIDTH), WIDTH ** -0.5, 0.09375, ((0, 32), (1, 8))),
        "code_weight": scatter_about(streams_of[6], (WIDTH, GATE_RANK), WIDTH ** -0.5, 0.09375, ((0, 32),)),
        "decay_weight": scatter_about(streams_of[7], (GATE_RANK, KEY_WIDTH), 1 ** -0.5, 6.0, ((1, 8),)),
        "decay_bias": jnp.clip(-4.0 + 6.0 * jax.random.uniform(streams_of[8], (KEY_WIDTH,), jnp.float32) ** levels(streams_of[8], (KEY_WIDTH,), ((0, 8),), -0.2, 0.2), -4.0, 2.0),
        "head_gain": jnp.clip(1.0 + 0.18 * jax.random.normal(streams_of[9], (VALUE_DIM,), jnp.float32), 0.1, 1.9),
        "key_cache": scatter_about(streams_of[10], (BATCH_TOTAL, BLOCK_SPAN, HEAD_COUNT, KEY_DIM), 1.0, 6.0, ((0, 32), (2, 8))),
        "value_cache": scatter_about(streams_of[11], (BATCH_TOTAL, BLOCK_SPAN, HEAD_COUNT, VALUE_DIM), 1.0, 6.0, ((0, 32), (2, 8))),
        "decay_cache": draw_decay_cache(jax.random.fold_in(streams_of[20], 71), 0),
        "carried_state": scatter_about(streams_of[13], (BATCH_TOTAL, HEAD_COUNT, KEY_DIM, VALUE_DIM), 4.0, 24.0, ((0, 32), (1, 8)), jnp.float32),
        "lengths": ragged_sizes(streams_of[14], BATCH_TOTAL, BATCH_TOTAL * (13 * BLOCK_SPAN // 32), BLOCK_SPAN, 2).astype(jnp.int32),
        "output_weight": scatter_about(streams_of[15], (VALUE_WIDTH, WIDTH), VALUE_WIDTH ** -0.5, 0.125, ((0, 8), (1, 32))),
        "mlp_gain": jnp.clip(1.0 + 0.18 * jax.random.normal(streams_of[16], (WIDTH,), jnp.float32), 0.1, 1.9),
        "gate_weight": scatter_about(streams_of[17], (WIDTH, MLP_WIDTH), WIDTH ** -0.5, 0.09375, ((0, 32), (1, 8))),
        "up_weight": scatter_about(streams_of[18], (WIDTH, MLP_WIDTH), WIDTH ** -0.5, 0.09375, ((0, 32), (1, 8))),
        "down_weight": scatter_about(streams_of[19], (MLP_WIDTH, WIDTH), MLP_WIDTH ** -0.5, 0.0546875, ((0, 8), (1, 32))),
    }


EPS = 1e-06
GATE_TEMP = 16.0

def block_attention(queries, new_keys, new_values, new_decay, key_cache, value_cache, decay_cache, carried_state, lengths):
    positions = jnp.arange(key_cache.shape[1], dtype=jnp.int32)
    live_mask = positions[None, :] < lengths[:, None]
    kept_decay = jnp.where(live_mask[:, :, None, None], decay_cache, jnp.zeros_like(decay_cache))
    later_sum = lax.cumsum(kept_decay, axis=1, reverse=True) - kept_decay
    total_decay = lax.optimization_barrier(jnp.sum(kept_decay, axis=1))
    decayed = queries.astype(jnp.float32) * jnp.exp(new_decay)
    carried = jnp.einsum('bhd,bhde->bhe', decayed * jnp.exp(total_decay), carried_state, precision=lax.Precision.HIGHEST)
    keyed_cache = key_cache.astype(jnp.float32) * jnp.exp(later_sum)
    scores = jnp.einsum('bhd,bshd->bhs', decayed, keyed_cache, precision=lax.Precision.HIGHEST)
    scores = jnp.where(live_mask[:, None, :], scores, jnp.zeros_like(scores)).astype(jnp.bfloat16)
    within = jnp.einsum('bhs,bshe->bhe', scores.astype(jnp.float32), value_cache.astype(jnp.float32))
    own_score = lax.optimization_barrier(jnp.sum(queries.astype(jnp.float32) * new_keys.astype(jnp.float32), axis=-1))
    return carried + within + own_score[..., None] * new_values.astype(jnp.float32)

def summed_by_group(left, weight, groups):
    row_count, inner_dim = left.shape
    group_parts = jnp.einsum('bni,nid->bnd', left.reshape(row_count, groups, inner_dim // groups).astype(jnp.float32), weight.reshape(groups, inner_dim // groups, weight.shape[1]).astype(jnp.float32))
    group_parts = lax.optimization_barrier(group_parts.astype(jnp.bfloat16))
    return lax.optimization_barrier(jnp.sum(group_parts.astype(jnp.float32), axis=1))

def reference(tokens, attn_gain, query_weight, key_weight, value_weight, outgate_weight, code_weight, decay_weight, decay_bias, head_gain, key_cache, value_cache, decay_cache, carried_state, lengths, output_weight, mlp_gain, gate_weight, up_weight, down_weight):
    token_f = tokens.astype(jnp.float32)
    scaled = (token_f * attn_gain[None, :]).astype(jnp.bfloat16)
    inv_rms = lax.rsqrt(lax.optimization_barrier(jnp.mean(token_f * token_f, axis=1, keepdims=True)) + EPS)

    def project(weight):
        return jnp.dot(scaled, weight, preferred_element_type=jnp.float32) * inv_rms
    queries = (project(query_weight) * KEY_DIM ** (-0.5)).astype(jnp.bfloat16).reshape(BATCH_TOTAL, HEAD_COUNT, KEY_DIM)
    new_keys = project(key_weight).astype(jnp.bfloat16).reshape(BATCH_TOTAL, HEAD_COUNT, KEY_DIM)
    new_values = project(value_weight).astype(jnp.bfloat16).reshape(BATCH_TOTAL, HEAD_COUNT, VALUE_DIM)
    out_gate = project(outgate_weight).astype(jnp.bfloat16).reshape(BATCH_TOTAL, HEAD_COUNT, VALUE_DIM)
    gate_code = project(code_weight).astype(jnp.bfloat16)
    pre_gate = jnp.dot(gate_code, decay_weight, preferred_element_type=jnp.float32) + decay_bias[None, :]
    new_decay = (jax.nn.log_sigmoid(pre_gate) / GATE_TEMP).reshape(BATCH_TOTAL, HEAD_COUNT, KEY_DIM)
    mixed_heads = block_attention(queries, new_keys, new_values, new_decay, key_cache, value_cache, decay_cache, carried_state, lengths)
    normed = mixed_heads * lax.rsqrt(lax.optimization_barrier(jnp.mean(mixed_heads * mixed_heads, axis=-1, keepdims=True)) + EPS) * head_gain
    heads_out = (normed * jax.nn.silu(out_gate.astype(jnp.float32))).astype(jnp.bfloat16).reshape(BATCH_TOTAL, HEAD_COUNT * VALUE_DIM)
    attended = summed_by_group(heads_out, output_weight, N_TP)
    middle = (token_f + attended).astype(jnp.bfloat16)
    mid_f = middle.astype(jnp.float32)
    scaled_mid = (mid_f * mlp_gain[None, :]).astype(jnp.bfloat16)
    inv_mid = lax.rsqrt(lax.optimization_barrier(jnp.mean(mid_f * mid_f, axis=1, keepdims=True)) + EPS)
    gate_act = jnp.dot(scaled_mid, gate_weight, preferred_element_type=jnp.float32) * inv_mid
    up_act = jnp.dot(scaled_mid, up_weight, preferred_element_type=jnp.float32) * inv_mid
    hidden = (jax.nn.silu(gate_act) * up_act).astype(jnp.bfloat16)
    lifted = summed_by_group(hidden, down_weight, N_TP)
    layer_out = (mid_f + lifted).astype(jnp.bfloat16)
    return (layer_out, new_keys, new_values)
```

```python
import jax
import jax.numpy as jnp
from jax import lax
from jax.sharding import Mesh
from jax.sharding import PartitionSpec as P

WIDTH = 4096
KV = ("z", "y")
TP = ("x", "c")


EPS = 1e-06
GATE_TEMP = 16.0


def sent_to_all(x, axis):
    length = lax.axis_size(axis)
    return lax.all_to_all(jnp.broadcast_to(x[None], (length, *x.shape)), axis, 0, 0, tiled=True)


def taken_together(x, axis):
    everything = sent_to_all(x, axis)
    return jnp.sum(everything.astype(jnp.float32), axis=0)


def split_up(x, dim, length):
    dims = x.shape
    tiles = x.reshape(*dims[:dim], length, dims[dim] // length, *dims[dim + 1 :])
    return jnp.moveaxis(tiles, dim, 0)


def sent_and_summed(x, axis, dim):
    length = lax.axis_size(axis)
    tiles = lax.all_to_all(split_up(x, dim, length), axis, 0, 0, tiled=True)
    return jnp.sum(tiles.astype(jnp.float32), axis=0)


def side_by_side(arrays, axis, dim, along):
    columns = [a.reshape(*a.shape[:along], -1) for a in arrays]
    both = jnp.concatenate(columns, axis=along)
    out, at, done = (sent_and_summed(both, axis, dim), 0, [])
    for a, column in zip(arrays, columns):
        share = out[..., at : at + column.shape[along]]
        done.append(share.reshape(*share.shape[:along], *a.shape[along:]))
        at += column.shape[along]
    return tuple(done)


def joined_along(tiles, dim):
    tiles = jnp.moveaxis(tiles, 0, dim)
    dims = tiles.shape
    return tiles.reshape(*dims[:dim], dims[dim] * dims[dim + 1], *dims[dim + 2 :])


def gathered_copies(x, axis, dim):
    tiles = sent_to_all(x, axis)
    return joined_along(tiles, dim)


def moved(x, axis, shift):
    length = lax.axis_size(axis)
    return lax.ppermute(x, axis, [(i, (i + shift) % length) for i in range(length)])


def across_heads(partial_value):
    mine = partial_value.astype(jnp.bfloat16)
    pair = mine.astype(jnp.float32) + moved(mine, "c", 1).astype(jnp.float32)
    sent = pair.astype(jnp.bfloat16)
    after, before, across = [moved(sent, "x", k).astype(jnp.float32) for k in (1, 3, 2)]
    return (sent.astype(jnp.float32) + across) + (after + before)


def block_attention(
    queries,
    new_keys,
    new_values,
    new_decay,
    key_cache,
    value_cache,
    decay_cache,
    carried_state,
    lengths,
):
    positions = jnp.arange(key_cache.shape[1], dtype=jnp.int32)
    live_mask = positions[None, :] < lengths[:, None]
    kept_decay = jnp.where(live_mask[:, :, None, None], decay_cache, jnp.zeros_like(decay_cache))
    later_sum = lax.cumsum(kept_decay, axis=1, reverse=True) - kept_decay
    total_decay = jnp.sum(kept_decay, axis=1)
    decayed = queries.astype(jnp.float32) * jnp.exp(new_decay)
    carried = jnp.einsum("bhd,bhde->bhe", decayed * jnp.exp(total_decay), carried_state)
    keyed_cache = key_cache.astype(jnp.float32) * jnp.exp(later_sum)
    scores = jnp.einsum("bhd,bshd->bhs", decayed, keyed_cache)
    scores = jnp.where(live_mask[:, None, :], scores, jnp.zeros_like(scores)).astype(jnp.bfloat16)
    within = jnp.einsum("bhs,bshe->bhe", scores, value_cache, preferred_element_type=jnp.float32)
    own_score = jnp.sum(queries.astype(jnp.float32) * new_keys.astype(jnp.float32), axis=-1)
    return carried + within + own_score[..., None] * new_values.astype(jnp.float32)


def mixer_hidden(gate_sum, up_sum, square_sum):
    inv_mid = lax.rsqrt(square_sum / WIDTH + EPS)[:, None]
    return (jax.nn.silu(gate_sum * inv_mid) * (up_sum * inv_mid)).astype(jnp.bfloat16)


def on_device(
    tokens,
    attn_gain,
    query_weight,
    key_weight,
    value_weight,
    outgate_weight,
    code_weight,
    decay_weight,
    decay_bias,
    head_gain,
    key_cache,
    value_cache,
    decay_cache,
    carried_state,
    lengths,
    output_weight,
    mlp_gain,
    gate_weight,
    up_weight,
    down_weight,
):
    local_seqs, heads_here, key_dim, value_dim = carried_state.shape
    token_f = tokens.astype(jnp.float32)
    scaled = (token_f * attn_gain[None, :]).astype(jnp.bfloat16)
    query_part = jnp.dot(scaled, query_weight, preferred_element_type=jnp.float32)
    key_part = jnp.dot(scaled, key_weight, preferred_element_type=jnp.float32)
    value_part = jnp.dot(scaled, value_weight, preferred_element_type=jnp.float32)
    outgate_part = jnp.dot(scaled, outgate_weight, preferred_element_type=jnp.float32)
    code_part = jnp.dot(scaled, code_weight, preferred_element_type=jnp.float32)
    token_squares = jnp.sum(token_f * token_f, axis=1)
    query_sum, key_sum, value_sum, outgate_sum, code_sum, square_sum = side_by_side(
        (
            query_part.astype(jnp.bfloat16),
            key_part.astype(jnp.bfloat16),
            value_part.astype(jnp.bfloat16),
            outgate_part.astype(jnp.bfloat16),
            code_part.astype(jnp.bfloat16),
            token_squares.astype(jnp.bfloat16),
        ),
        KV,
        0,
        1,
    )
    inv_rms = lax.rsqrt(square_sum / WIDTH + EPS)[:, None]
    queries = (
        (query_sum * inv_rms * key_dim ** (-0.5))
        .astype(jnp.bfloat16)
        .reshape(local_seqs, heads_here, key_dim)
    )
    new_keys = (key_sum * inv_rms).astype(jnp.bfloat16).reshape(local_seqs, heads_here, key_dim)
    new_values = (
        (value_sum * inv_rms).astype(jnp.bfloat16).reshape(local_seqs, heads_here, value_dim)
    )
    out_gate = (
        (outgate_sum * inv_rms).astype(jnp.bfloat16).reshape(local_seqs, heads_here, value_dim)
    )
    gate_code = (code_sum * inv_rms).astype(jnp.bfloat16)
    pre_gate = (
        jnp.dot(gate_code, decay_weight, preferred_element_type=jnp.float32) + decay_bias[None, :]
    )
    new_decay = (jax.nn.log_sigmoid(pre_gate) / GATE_TEMP).reshape(local_seqs, heads_here, key_dim)
    mixed_heads = block_attention(
        queries,
        new_keys,
        new_values,
        new_decay,
        key_cache,
        value_cache,
        decay_cache,
        carried_state,
        lengths,
    )
    normed = (
        mixed_heads
        * lax.rsqrt(jnp.mean(mixed_heads * mixed_heads, axis=-1, keepdims=True) + EPS)
        * head_gain
    )
    heads_out = (
        (normed * jax.nn.silu(out_gate.astype(jnp.float32)))
        .astype(jnp.bfloat16)
        .reshape(local_seqs, heads_here * value_dim)
    )
    attended = across_heads(
        jnp.dot(
            gathered_copies(heads_out, KV, 0), output_weight, preferred_element_type=jnp.float32
        )
    )
    middle = (token_f + attended).astype(jnp.bfloat16)
    mid_f = middle.astype(jnp.float32)
    scaled_mid = (mid_f * mlp_gain[None, :]).astype(jnp.bfloat16)
    gate_part = jnp.dot(scaled_mid, gate_weight, preferred_element_type=jnp.float32)
    up_part = jnp.dot(scaled_mid, up_weight, preferred_element_type=jnp.float32)
    mid_squares = jnp.sum(mid_f * mid_f, axis=1)
    gate_sum, up_sum, mid_sum = side_by_side(
        (
            gate_part.astype(jnp.bfloat16),
            up_part.astype(jnp.bfloat16),
            mid_squares.astype(jnp.bfloat16),
        ),
        KV,
        0,
        1,
    )
    hidden_share = mixer_hidden(gate_sum, up_sum, mid_sum)
    lifted_part = jnp.dot(
        gathered_copies(hidden_share, KV, 0), down_weight, preferred_element_type=jnp.float32
    )
    layer_out = (mid_f + across_heads(lifted_part)).astype(jnp.bfloat16)
    return (layer_out, new_keys, new_values)


def solution(mesh):
    axes = Mesh(mesh.devices.reshape(8, 4, 4, 2), ("z", "y", "x", "c"))
    in_specs = (
        P(None, KV),
        P(KV),
        P(KV, TP),
        P(KV, TP),
        P(KV, TP),
        P(KV, TP),
        P(KV, None),
        P(None, TP),
        P(TP),
        P(),
        P(KV, None, TP, None),
        P(KV, None, TP, None),
        P(KV, None, TP, None),
        P(KV, TP, None, None),
        P(KV),
        P(TP, KV),
        P(KV),
        P(KV, TP),
        P(KV, TP),
        P(TP, KV),
    )
    out_specs = (P(None, KV), P(KV, TP, None), P(KV, TP, None))
    return jax.shard_map(
        on_device, mesh=axes, in_specs=in_specs, out_specs=out_specs, check_vma=False
    )
```

```python
import functools

import jax
import jax.numpy as jnp
from jax import lax
from jax.experimental import pallas as pl
from jax.experimental.pallas import tpu as pltpu
from jax.sharding import Mesh
from jax.sharding import PartitionSpec as P

WIDTH = 4096
EPS = 1e-06
GATE_TEMP = 16.0
KV = ("z", "y")
TP = ("x", "c")
F32 = jnp.float32
BF16 = jnp.bfloat16
FIRST = 512
CODE_AT = 256
SQUARE_AT = 272
UNITS = 1376
SECOND = 1408


def kernel(body, outs, name):
    return pl.pallas_call(
        body,
        out_shape=tuple(jax.ShapeDtypeStruct(shape, dtype) for shape, dtype in outs),
        name=name,
    )


def store_shares(out_ref, low, high, at=0):
    rows, width = low.shape
    low = low.reshape(rows // 8, 8, width)
    high = high.reshape(rows // 8, 8, width)
    first = lax.broadcasted_iota(jnp.int32, low.shape, 1) < 4
    out_ref[:, 0, :, at : at + width] = jnp.where(first, low, pltpu.roll(high, 4, 1)).astype(BF16)
    out_ref[:, 1, :, at : at + width] = jnp.where(first, pltpu.roll(low, 4, 1), high).astype(BF16)


def dot(a, b, dims=((1,), (0,)), **kw):
    return lax.dot_general(a, b, (dims, ((), ())), preferred_element_type=F32, **kw)


def project_body(tok_ref, gain_ref, q_ref, k_ref, v_ref, g_ref, code_ref, out_ref):
    tok = tok_ref[...].astype(F32)
    scaled = (tok * gain_ref[...]).astype(BF16)
    squares = jnp.sum(tok * tok, axis=1, keepdims=True)
    code = dot(scaled, code_ref[...], ((1,), (1,)))
    lane = lax.broadcasted_iota(jnp.int32, (128, 256), 1)
    tail = jnp.concatenate([code, jnp.zeros((128, 240), F32)], axis=1)
    tail = jnp.where(lane == SQUARE_AT - CODE_AT, squares, tail)
    out_gate = dot(scaled, g_ref[...])
    head = jnp.concatenate([dot(scaled, q_ref[...]), dot(scaled, k_ref[...])], axis=1)
    store_shares(out_ref, head, out_gate)
    store_shares(out_ref, dot(scaled, v_ref[...]), tail, 256)


def rounded(x):
    return x.astype(BF16).astype(F32)


def attend_body(
    got_ref, dw_ref, bias_ref, hg_ref, key_ref, value_ref, decay_ref, state_ref, len_ref,
    heads_ref, nk_ref, nv_ref,
):
    total = jnp.sum(got_ref[...].astype(F32), axis=0)
    squares = jnp.broadcast_to(total[:, SQUARE_AT : SQUARE_AT + 1], (8, 128))
    inv_high = lax.rsqrt(squares / WIDTH + EPS)
    inv_low = pltpu.roll(inv_high, 4, 0)
    twice = lambda x: jnp.concatenate([x, x], axis=1)
    queries = rounded(total[:, 0:128] * inv_low * 128 ** (-0.5))
    keys = (total[:, 128:256] * inv_low).astype(BF16)
    values = (total[:, 256:512] * twice(inv_low)).astype(BF16)
    out_gate = pltpu.roll(rounded(total[:, 0:256] * twice(inv_high)), 4, 0)
    code = (total[:, CODE_AT : CODE_AT + 128] * inv_high).astype(BF16)[:, 0:16]
    pre = pltpu.roll(dot(code, dw_ref[...]) + bias_ref[...], 4, 0)
    log_sig = jnp.minimum(pre, 0.0) - jnp.log1p(jnp.exp(-jnp.abs(pre)))
    decayed = queries * jnp.exp(log_sig / GATE_TEMP)
    own = jnp.sum(queries * keys.astype(F32), axis=1, keepdims=True)
    row = lax.broadcasted_iota(jnp.int32, (64, 64), 0)
    col = lax.broadcasted_iota(jnp.int32, (64, 64), 1)
    later = (col > row).astype(F32)
    position = lax.broadcasted_iota(jnp.int32, (64, 128), 0)
    live = [position < len_ref[b] for b in range(4)]
    kept = [jnp.where(live[b], decay_ref[b], 0.0) for b in range(4)]
    sums = dot(later, jnp.concatenate(kept, axis=1), precision=lax.Precision.HIGHEST)
    totals = jnp.concatenate([jnp.sum(k, axis=0, keepdims=True) for k in kept], axis=0)
    carry = decayed[0:4] * jnp.exp(totals)
    columns = jnp.concatenate([carry, carry], axis=0).T
    mixed = []
    for b in range(4):
        keyed = key_ref[b].astype(F32) * jnp.exp(sums[:, 128 * b : 128 * b + 128])
        scores = jnp.sum(jnp.where(live[b], keyed * decayed[b : b + 1], 0.0), axis=1, keepdims=True)
        within = jnp.sum(rounded(scores) * value_ref[b].astype(F32), axis=0, keepdims=True)
        carried = jnp.sum(columns[:, b : b + 1] * state_ref[b], axis=0, keepdims=True)
        mixed.append(carried + within)
    mixed = jnp.concatenate(mixed, axis=0) + own[0:4] * values[0:4].astype(F32)
    scale = lax.rsqrt(jnp.mean(mixed * mixed, axis=1, keepdims=True) + EPS)
    gate = out_gate[0:4]
    heads_ref[...] = (mixed * scale * hg_ref[...] * (gate / (1.0 + jnp.exp(-gate)))).astype(BF16)
    nk_ref[...] = keys[0:4]
    nv_ref[...] = values[0:4]


def lift_body(tok_ref, gain_ref, mine_ref, after_ref, before_ref, across_ref, gate_ref, up_ref, mid_ref, out_ref):
    attended = (mine_ref[...].astype(F32) + across_ref[...].astype(F32)) + (
        after_ref[...].astype(F32) + before_ref[...].astype(F32)
    )
    middle = (tok_ref[...].astype(F32) + attended).astype(BF16)
    mid_ref[...] = middle
    mid = middle.astype(F32)
    scaled = (mid * gain_ref[...]).astype(BF16)
    squares = jnp.sum(mid * mid, axis=1, keepdims=True)
    for at, width in ((0, 512), (512, 512), (1024, 384)):
        real = min(width, UNITS - at)
        low = dot(scaled, gate_ref[at : at + real, :], ((1,), (1,)))
        high = dot(scaled, up_ref[at : at + real, :], ((1,), (1,)))
        if real < width:
            pad = jnp.broadcast_to(squares, (128, width - real))
            low = jnp.concatenate([low, pad], axis=1)
            high = jnp.concatenate([high, pad], axis=1)
        store_shares(out_ref, low, high, at)


def hidden_body(got_ref, out_ref):
    total = jnp.sum(got_ref[...].astype(F32), axis=0)
    inv = lax.rsqrt(total[0:4, UNITS : UNITS + 1] / WIDTH + EPS)
    gate = total[0:4] * inv
    up = pltpu.roll(total, 4, 0)[0:4] * inv
    out_ref[...] = (gate / (1.0 + jnp.exp(-gate)) * up).astype(BF16)


def down_body(hidden_ref, down_ref, out_ref):
    out_ref[...] = dot(hidden_ref[:, 0:UNITS], down_ref[...]).astype(BF16)


def out_body(heads_ref, weight_ref, out_ref):
    out_ref[...] = dot(heads_ref[...], weight_ref[...]).astype(BF16)


def moved(x, axis, shift):
    length = lax.axis_size(axis)
    return lax.ppermute(x, axis, [(i, (i + shift) % length) for i in range(length)])


def tp_parts(mine):
    pair = (mine.astype(F32) + moved(mine, "c", 1).astype(F32)).astype(BF16)
    return (pair, *(moved(pair, "x", k) for k in (1, 3, 2)))


def to_all(x):
    devices = lax.axis_size(KV)
    copies = jnp.broadcast_to(x[None], (devices, *x.shape))
    got = lax.all_to_all(copies, KV, 0, 0, tiled=True)
    return got.reshape(devices * x.shape[0], x.shape[1])


def shares(x):
    return lax.all_to_all(x.reshape(32, 8, x.shape[-1]), KV, 0, 0, tiled=True)


def on_device(
    tokens,
    attn_gain,
    query_weight,
    key_weight,
    value_weight,
    outgate_weight,
    code_weight,
    decay_weight,
    decay_bias,
    head_gain,
    key_cache,
    value_cache,
    decay_cache,
    carried_state,
    lengths,
    output_weight,
    mlp_gain,
    gate_weight,
    up_weight,
    down_weight,
):
    seqs = key_cache.shape[0]
    (first,) = kernel(project_body, [((16, 2, 8, FIRST), BF16)], "project")(
        tokens, attn_gain[None], query_weight, key_weight, value_weight, outgate_weight, code_weight.T
    )
    heads, new_keys, new_values = pl.pallas_call(
        attend_body,
        out_shape=(
            jax.ShapeDtypeStruct((seqs, 256), BF16),
            jax.ShapeDtypeStruct((seqs, 128), BF16),
            jax.ShapeDtypeStruct((seqs, 256), BF16),
        ),
        in_specs=[pl.BlockSpec(memory_space=pltpu.VMEM)] * 8 + [pl.BlockSpec(memory_space=pltpu.SMEM)],
        name="attend",
    )(
        shares(first),
        decay_weight,
        decay_bias[None],
        head_gain[None],
        key_cache[:, :, 0],
        value_cache[:, :, 0],
        decay_cache[:, :, 0],
        carried_state[:, 0],
        lengths,
    )
    (attended,) = kernel(out_body, [((128, 128), BF16)], "attended")(to_all(heads), output_weight)
    middle, second = kernel(
        lift_body, [((128, 128), BF16), ((16, 2, 8, SECOND), BF16)], "lift"
    )(tokens, mlp_gain[None], *tp_parts(attended), gate_weight.T, up_weight.T)
    (hidden,) = kernel(hidden_body, [((4, SECOND), BF16)], "hidden")(shares(second))
    (lifted,) = kernel(down_body, [((128, 128), BF16)], "down")(to_all(hidden), down_weight)
    mine, after, before, across = (part.astype(F32) for part in tp_parts(lifted))
    layer_out = (middle.astype(F32) + ((mine + across) + (after + before))).astype(BF16)
    return (layer_out, new_keys[:, None], new_values[:, None])


def solution(mesh):
    axes = Mesh(mesh.devices.reshape(8, 4, 4, 2), ("z", "y", "x", "c"))
    in_specs = (
        P(None, KV),
        P(KV),
        P(KV, TP),
        P(KV, TP),
        P(KV, TP),
        P(KV, TP),
        P(KV, None),
        P(None, TP),
        P(TP),
        P(),
        P(KV, None, TP, None),
        P(KV, None, TP, None),
        P(KV, None, TP, None),
        P(KV, TP, None, None),
        P(KV),
        P(TP, KV),
        P(KV),
        P(KV, TP),
        P(KV, TP),
        P(TP, KV),
    )
    out_specs = (P(None, KV), P(KV, TP, None), P(KV, TP, None))
    return jax.shard_map(
        on_device, mesh=axes, in_specs=in_specs, out_specs=out_specs, check_vma=False
    )
```

```python
import jax
import jax.numpy as jnp
from jax import lax
from jax.experimental import pallas as pl
from jax.experimental.pallas import tpu as pltpu
from jax.sharding import Mesh
from jax.sharding import PartitionSpec as P

WIDTH = 4096
EPS = 1e-06
GATE_TEMP = 16.0
KV = ("z", "y")
TP = ("x", "c")
F32 = jnp.float32
BF16 = jnp.bfloat16
FIRST = 512
CODE_AT = 256
SQUARE_AT = 272
UNITS = 1376
SECOND = 1408


def kernel(body, outs, name, args, fetched=()):
    count, own, more = len(args), len(outs), len(fetched)

    def whole(*refs):
        from_refs = refs[count : count + more]
        out_refs = refs[count + more : -1] if more else refs[count:]
        copies = [
            pltpu.make_async_copy(source, target, refs[-1].at[k])
            for k, (source, target) in enumerate(zip(from_refs, out_refs[own:]))
        ]
        for copy in copies:
            copy.start()
        body(*refs[:count], *out_refs[:own])
        for copy in copies:
            copy.wait()

    return pl.pallas_call(
        whole,
        out_shape=tuple(pltpu.VMEM(*out) for out in (*outs, *((a.shape, a.dtype) for a in fetched))),
        in_specs=[pl.BlockSpec(memory_space=pltpu.VMEM)] * count + [pl.BlockSpec(memory_space=pl.ANY)] * more,
        out_specs=[pl.BlockSpec(memory_space=pltpu.VMEM)] * (own + more),
        scratch_shapes=[pltpu.SemaphoreType.DMA((more,))] if more else [],
        compiler_params=pltpu.CompilerParams(vmem_limit_bytes=8 << 20),
        name=name,
    )(*args, *map(in_hbm, fetched))


def in_hbm(x):
    return pltpu.with_memory_space_constraint(x, pltpu.HBM)


def store_shares(out_ref, low, high, at=0):
    rows, width = low.shape
    low = low.reshape(rows // 8, 8, width)
    high = high.reshape(rows // 8, 8, width)
    first = lax.broadcasted_iota(jnp.int32, low.shape, 1) < 4
    out_ref[:, 0, :, at : at + width] = jnp.where(first, low, pltpu.roll(high, 4, 1)).astype(BF16)
    out_ref[:, 1, :, at : at + width] = jnp.where(first, pltpu.roll(low, 4, 1), high).astype(BF16)


def dot(a, b, dims=((1,), (0,)), **kw):
    return lax.dot_general(a, b, (dims, ((), ())), preferred_element_type=F32, **kw)


def project_body(tok_ref, gain_ref, q_ref, k_ref, v_ref, g_ref, code_ref, out_ref, tok_out_ref):
    tok_out_ref[...] = tok_ref[...]
    tok = tok_ref[...].astype(F32)
    scaled = (tok * gain_ref[...]).astype(BF16)
    squares = jnp.sum(tok * tok, axis=1, keepdims=True)
    code = dot(scaled, code_ref[...], ((1,), (1,)))
    lane = lax.broadcasted_iota(jnp.int32, (128, 256), 1)
    tail = jnp.concatenate([code, jnp.zeros((128, 240), F32)], axis=1)
    tail = jnp.where(lane == SQUARE_AT - CODE_AT, squares, tail)
    out_gate = dot(scaled, g_ref[...])
    head = jnp.concatenate([dot(scaled, q_ref[...]), dot(scaled, k_ref[...])], axis=1)
    store_shares(out_ref, head, out_gate)
    store_shares(out_ref, dot(scaled, v_ref[...]), tail, 256)


def rounded(x):
    return x.astype(BF16).astype(F32)


def attend_body(
    got_ref, dw_ref, bias_ref, hg_ref, len_ref, key_ref, value_ref, decay_ref, state_ref,
    heads_ref, nk_ref, nv_ref,
):
    total = jnp.sum(got_ref[...].astype(F32), axis=0)
    squares = jnp.broadcast_to(total[:, SQUARE_AT : SQUARE_AT + 1], (8, 128))
    inv_high = lax.rsqrt(squares / WIDTH + EPS)
    inv_low = pltpu.roll(inv_high, 4, 0)
    twice = lambda x: jnp.concatenate([x, x], axis=1)
    queries = rounded(total[:, 0:128] * inv_low * 128 ** (-0.5))
    keys = (total[:, 128:256] * inv_low).astype(BF16)
    values = (total[:, 256:512] * twice(inv_low)).astype(BF16)
    out_gate = pltpu.roll(rounded(total[:, 0:256] * twice(inv_high)), 4, 0)
    code = (total[:, CODE_AT : CODE_AT + 128] * inv_high).astype(BF16)[:, 0:16]
    pre = pltpu.roll(dot(code, dw_ref[...]) + bias_ref[...], 4, 0)
    log_sig = jnp.minimum(pre, 0.0) - jnp.log1p(jnp.exp(-jnp.abs(pre)))
    decayed = queries * jnp.exp(log_sig / GATE_TEMP)
    own = jnp.sum(queries * keys.astype(F32), axis=1, keepdims=True)
    row = lax.broadcasted_iota(jnp.int32, (64, 64), 0)
    col = lax.broadcasted_iota(jnp.int32, (64, 64), 1)
    later = (col > row).astype(F32)
    position = lax.broadcasted_iota(jnp.int32, (64, 128), 0)
    live = [position < len_ref[:, b : b + 1] for b in range(4)]
    kept = [jnp.where(live[b], decay_ref[b], 0.0) for b in range(4)]
    sums = dot(later, jnp.concatenate(kept, axis=1), precision=lax.Precision.HIGHEST)
    totals = jnp.concatenate([jnp.sum(k, axis=0, keepdims=True) for k in kept], axis=0)
    carry = decayed[0:4] * jnp.exp(totals)
    columns = jnp.concatenate([carry, carry], axis=0).T
    mixed = []
    for b in range(4):
        keyed = key_ref[b].astype(F32) * jnp.exp(sums[:, 128 * b : 128 * b + 128])
        scores = jnp.sum(jnp.where(live[b], keyed * decayed[b : b + 1], 0.0), axis=1, keepdims=True)
        within = jnp.sum(rounded(scores) * value_ref[b].astype(F32), axis=0, keepdims=True)
        carried = jnp.sum(columns[:, b : b + 1] * state_ref[b], axis=0, keepdims=True)
        mixed.append(carried + within)
    mixed = jnp.concatenate(mixed, axis=0) + own[0:4] * values[0:4].astype(F32)
    scale = lax.rsqrt(jnp.mean(mixed * mixed, axis=1, keepdims=True) + EPS)
    gate = out_gate[0:4]
    heads_ref[...] = (mixed * scale * hg_ref[...] * (gate / (1.0 + jnp.exp(-gate)))).astype(BF16)
    nk_ref[...] = keys[0:4]
    nv_ref[...] = values[0:4]


def lift_body(tok_ref, gain_ref, mine_ref, after_ref, before_ref, across_ref, gate_ref, up_ref, mid_ref, out_ref):
    attended = (mine_ref[...].astype(F32) + across_ref[...].astype(F32)) + (
        after_ref[...].astype(F32) + before_ref[...].astype(F32)
    )
    middle = (tok_ref[...].astype(F32) + attended).astype(BF16)
    mid_ref[...] = middle
    mid = middle.astype(F32)
    scaled = (mid * gain_ref[...]).astype(BF16)
    squares = jnp.sum(mid * mid, axis=1, keepdims=True)
    for at, width in ((0, 512), (512, 512), (1024, 384)):
        real = min(width, UNITS - at)
        low = dot(scaled, gate_ref[at : at + real, :], ((1,), (1,)))
        high = dot(scaled, up_ref[at : at + real, :], ((1,), (1,)))
        if real < width:
            pad = jnp.broadcast_to(squares, (128, width - real))
            low = jnp.concatenate([low, pad], axis=1)
            high = jnp.concatenate([high, pad], axis=1)
        store_shares(out_ref, low, high, at)


def hidden_body(got_ref, out_ref):
    total = jnp.sum(got_ref[...].astype(F32), axis=0)
    inv = lax.rsqrt(total[0:4, UNITS : UNITS + 1] / WIDTH + EPS)
    gate = total[0:4] * inv
    up = pltpu.roll(total, 4, 0)[0:4] * inv
    out_ref[...] = (gate / (1.0 + jnp.exp(-gate)) * up).astype(BF16)


def down_body(hidden_ref, down_ref, out_ref):
    out_ref[...] = dot(hidden_ref[:, 0:UNITS], down_ref[...]).astype(BF16)


def out_body(heads_ref, weight_ref, out_ref):
    out_ref[...] = dot(heads_ref[...], weight_ref[...]).astype(BF16)


def moved(x, axis, shift):
    length = lax.axis_size(axis)
    return lax.ppermute(x, axis, [(i, (i + shift) % length) for i in range(length)])


def tp_parts(mine):
    pair = (mine.astype(F32) + moved(mine, "c", 1).astype(F32)).astype(BF16)
    return (pair, *(moved(pair, "x", k) for k in (1, 3, 2)))


def to_all(x):
    devices = lax.axis_size(KV)
    copies = jnp.broadcast_to(x[None], (devices, *x.shape))
    got = lax.all_to_all(copies, KV, 0, 0, tiled=True)
    return got.reshape(devices * x.shape[0], x.shape[1])


def shares(x):
    return lax.all_to_all(x.reshape(32, 8, x.shape[-1]), KV, 0, 0, tiled=True)


def on_device(
    tokens,
    attn_gain,
    query_weight,
    key_weight,
    value_weight,
    outgate_weight,
    code_weight,
    decay_weight,
    decay_bias,
    head_gain,
    key_cache,
    value_cache,
    decay_cache,
    carried_state,
    lengths,
    output_weight,
    mlp_gain,
    gate_weight,
    up_weight,
    down_weight,
):
    seqs = key_cache.shape[0]
    read = (tokens, attn_gain[None], query_weight, key_weight, value_weight, outgate_weight, code_weight.T)
    first, tokens, mlp_gain, *small, key_cache = kernel(
        project_body,
        [((16, 2, 8, FIRST), BF16), (tokens.shape, BF16)],
        "project",
        [in_hbm(a) for a in read],
        (mlp_gain[None], decay_weight, decay_bias[None], head_gain[None], lengths[None], key_cache[:, :, 0]),
    )
    heads, new_keys, new_values, down_weight = kernel(
        attend_body,
        [((seqs, 256), BF16), ((seqs, 128), BF16), ((seqs, 256), BF16)],
        "attend",
        (shares(first), *small, key_cache, value_cache[:, :, 0], decay_cache[:, :, 0], carried_state[:, 0]),
        (down_weight,),
    )
    (attended,) = kernel(out_body, [((128, 128), BF16)], "attended", (to_all(heads), output_weight))
    middle, second = kernel(
        lift_body,
        [((128, 128), BF16), ((16, 2, 8, SECOND), BF16)],
        "lift",
        (tokens, mlp_gain, *tp_parts(attended), gate_weight.T, up_weight.T),
    )
    (hidden,) = kernel(hidden_body, [((seqs, SECOND), BF16)], "hidden", (shares(second),))
    (lifted,) = kernel(down_body, [((128, 128), BF16)], "down", (to_all(hidden), down_weight))
    mine, after, before, across = (part.astype(F32) for part in tp_parts(lifted))
    layer_out = (middle.astype(F32) + ((mine + across) + (after + before))).astype(BF16)
    return (layer_out, new_keys[:, None], new_values[:, None])


def solution(mesh):
    axes = Mesh(mesh.devices.reshape(8, 4, 4, 2), ("z", "y", "x", "c"))
    in_specs = (
        P(None, KV),
        P(KV),
        P(KV, TP),
        P(KV, TP),
        P(KV, TP),
        P(KV, TP),
        P(KV, None),
        P(None, TP),
        P(TP),
        P(),
        P(KV, None, TP, None),
        P(KV, None, TP, None),
        P(KV, None, TP, None),
        P(KV, TP, None, None),
        P(KV),
        P(TP, KV),
        P(KV),
        P(KV, TP),
        P(KV, TP),
        P(TP, KV),
    )
    out_specs = (P(None, KV), P(KV, TP, None), P(KV, TP, None))
    return jax.shard_map(
        on_device, mesh=axes, in_specs=in_specs, out_specs=out_specs, check_vma=False
    )
```

```python
import jax
import jax.numpy as jnp
from jax import lax
from jax.experimental import pallas as pl
from jax.experimental.pallas import tpu as pltpu
from jax.sharding import Mesh
from jax.sharding import PartitionSpec as P

WIDTH = 4096
EPS = 1e-06
GATE_TEMP = 16.0
KV = ("z", "y")
TP = ("x", "c")
F32 = jnp.float32
BF16 = jnp.bfloat16
FIRST = 512
CODE_AT = 256
SQUARE_AT = 272
TOKENS_AT = 256
GAIN_AT = 384
SENT = 400
UNITS = 1376
SECOND = 1408


def kernel(body, outs, args, fetched=()):
    count, more = len(args), len(fetched)

    def whole(*refs):
        arg_refs, from_refs = refs[:count], refs[count : count + more]
        out_refs = refs[count + more : -1] if more else refs[count:]
        copies = [
            pltpu.make_async_copy(
                source, out_refs[out].at[pl.ds(row, source.shape[0])], refs[-1].at[k]
            )
            for k, (source, (_, out, row)) in enumerate(zip(from_refs, fetched))
        ]
        for copy in copies:
            copy.start()
        body(*arg_refs, *out_refs)
        for copy in copies:
            copy.wait()

    return pl.pallas_call(
        whole,
        out_shape=tuple(pltpu.VMEM(*out) for out in outs),
        in_specs=[pl.BlockSpec(memory_space=pltpu.VMEM)] * count + [pl.BlockSpec(memory_space=pl.ANY)] * more,
        out_specs=[pl.BlockSpec(memory_space=pltpu.VMEM)] * len(outs),
        scratch_shapes=[pltpu.SemaphoreType.DMA((more,))] if more else [],
        compiler_params=pltpu.CompilerParams(vmem_limit_bytes=8 << 20),
    )(*args, *(in_hbm(array) for array, _, _ in fetched))


def in_hbm(x):
    return pltpu.with_memory_space_constraint(x, pltpu.HBM)


def store_shares(out_ref, low, high, at=0):
    rows, width = low.shape
    low = low.reshape(rows // 8, 8, width)
    high = high.reshape(rows // 8, 8, width)
    first = lax.broadcasted_iota(jnp.int32, low.shape, 1) < 4
    out_ref[:, 0, :, at : at + width] = jnp.where(first, low, pltpu.roll(high, 4, 1)).astype(BF16)
    out_ref[:, 1, :, at : at + width] = jnp.where(first, pltpu.roll(low, 4, 1), high).astype(BF16)


def dot(a, b, dims=((1,), (0,)), **kw):
    return lax.dot_general(a, b, (dims, ((), ())), preferred_element_type=F32, **kw)


def project_body(tok_ref, gain_ref, q_ref, k_ref, v_ref, g_ref, code_ref, mlp_gain_ref, out_ref, sent_ref, *_):
    part = mlp_gain_ref[...]
    rows = []
    for _ in range(3):
        rows.append(rounded(part))
        part = part - rows[-1]
    rows = jnp.concatenate([*rows, jnp.zeros((SENT - GAIN_AT - 3, 128), F32)], axis=0)
    sent_ref[GAIN_AT:SENT, :] = rows.astype(BF16)
    tok = tok_ref[...].astype(F32)
    scaled = (tok * gain_ref[...]).astype(BF16)
    squares = jnp.sum(tok * tok, axis=1, keepdims=True)
    code = dot(scaled, code_ref[...], ((1,), (1,)))
    lane = lax.broadcasted_iota(jnp.int32, (128, 256), 1)
    tail = jnp.concatenate([code, jnp.zeros((128, 240), F32)], axis=1)
    tail = jnp.where(lane == SQUARE_AT - CODE_AT, squares, tail)
    out_gate = dot(scaled, g_ref[...])
    head = jnp.concatenate([dot(scaled, q_ref[...]), dot(scaled, k_ref[...])], axis=1)
    store_shares(out_ref, head, out_gate)
    store_shares(out_ref, dot(scaled, v_ref[...]), tail, 256)


def rounded(x):
    return x.astype(BF16).astype(F32)


def attend_body(
    got_ref, dw_ref, bias_ref, hg_ref, len_ref, decay_hbm, key_hbm, value_hbm, state_hbm,
    heads_ref, nk_ref, nv_ref, decay_ref, key_ref, value_ref, state_ref, sems,
):
    sources = (decay_hbm, key_hbm, value_hbm, state_hbm)
    targets = (decay_ref, key_ref, value_ref, state_ref)
    copies = [pltpu.make_async_copy(a, b, sems.at[k]) for k, (a, b) in enumerate(zip(sources, targets))]
    for copy in copies:
        copy.start()
    total = jnp.sum(got_ref[...].astype(F32), axis=0)
    squares = jnp.broadcast_to(total[:, SQUARE_AT : SQUARE_AT + 1], (8, 128))
    inv_high = lax.rsqrt(squares / WIDTH + EPS)
    inv_low = pltpu.roll(inv_high, 4, 0)
    twice = lambda x: jnp.concatenate([x, x], axis=1)
    queries = rounded(total[:, 0:128] * inv_low * 128 ** (-0.5))
    keys = (total[:, 128:256] * inv_low).astype(BF16)
    values = (total[:, 256:512] * twice(inv_low)).astype(BF16)
    out_gate = pltpu.roll(rounded(total[:, 0:256] * twice(inv_high)), 4, 0)
    code = (total[:, CODE_AT : CODE_AT + 128] * inv_high).astype(BF16)[:, 0:16]
    pre = pltpu.roll(dot(code, dw_ref[...]) + bias_ref[...], 4, 0)
    log_sig = jnp.minimum(pre, 0.0) - jnp.log1p(jnp.exp(-jnp.abs(pre)))
    decayed = queries * jnp.exp(log_sig / GATE_TEMP)
    own = jnp.sum(queries * keys.astype(F32), axis=1, keepdims=True)
    row = lax.broadcasted_iota(jnp.int32, (64, 64), 0)
    col = lax.broadcasted_iota(jnp.int32, (64, 64), 1)
    later = (col > row).astype(F32)
    position = lax.broadcasted_iota(jnp.int32, (64, 128), 0)
    copies[0].wait()
    live = [position < len_ref[:, b : b + 1] for b in range(4)]
    kept = [jnp.where(live[b], decay_ref[b], 0.0) for b in range(4)]
    sums = dot(later, jnp.concatenate(kept, axis=1), precision=lax.Precision.HIGHEST)
    totals = jnp.concatenate([jnp.sum(k, axis=0, keepdims=True) for k in kept], axis=0)
    carry = decayed[0:4] * jnp.exp(totals)
    columns = jnp.concatenate([carry, carry], axis=0).T
    for copy in copies[1:]:
        copy.wait()
    mixed = []
    for b in range(4):
        keyed = key_ref[b].astype(F32) * jnp.exp(sums[:, 128 * b : 128 * b + 128])
        scores = jnp.sum(jnp.where(live[b], keyed * decayed[b : b + 1], 0.0), axis=1, keepdims=True)
        within = jnp.sum(rounded(scores) * value_ref[b].astype(F32), axis=0, keepdims=True)
        carried = jnp.sum(columns[:, b : b + 1] * state_ref[b], axis=0, keepdims=True)
        mixed.append(carried + within)
    mixed = jnp.concatenate(mixed, axis=0) + own[0:4] * values[0:4].astype(F32)
    scale = lax.rsqrt(jnp.mean(mixed * mixed, axis=1, keepdims=True) + EPS)
    gate = out_gate[0:4]
    heads_ref[...] = (mixed * scale * hg_ref[...] * (gate / (1.0 + jnp.exp(-gate)))).astype(BF16)
    nk_ref[...] = keys[0:4]
    nv_ref[...] = values[0:4]


def sequences_of(y, shape, dim):
    place = lax.broadcasted_iota(jnp.int32, shape, dim)
    group = place // 32
    owner = jnp.where(group == 0, y, jnp.where(group == 1, y + 3, jnp.where(group == 2, y + 1, y + 2))) % 4
    return (place % 32) // 4 * 16 + owner * 4 + place % 4


def chosen(condition):
    return jnp.where(condition, 1.0, 0.0).astype(BF16)


def lift_body(mine_ref, after_ref, before_ref, across_ref, *refs):
    sent_refs, weight_refs, (mid_ref, out_ref) = refs[:4], refs[4:8], refs[8:]
    attended = (mine_ref[...].astype(F32) + across_ref[...].astype(F32)) + (
        after_ref[...].astype(F32) + before_ref[...].astype(F32)
    )
    own = sequences_of(lax.axis_index("y"), (32, 128), 0)
    pick = chosen(own == lax.broadcasted_iota(jnp.int32, (32, 128), 1))
    tok = jnp.concatenate([dot(pick, ref[TOKENS_AT:GAIN_AT, :]) for ref in sent_refs], axis=1)
    middle = (tok + attended).astype(BF16)
    mid = middle.astype(F32)
    scaled = []
    for k, ref in enumerate(sent_refs):
        mid_ref[k] = middle[:, 128 * k : 128 * k + 128]
        gain = jnp.sum(ref[GAIN_AT:SENT, :].astype(F32), axis=0, keepdims=True)
        scaled.append((mid[:, 128 * k : 128 * k + 128] * gain).astype(BF16))
    squares = jnp.sum(mid * mid, axis=1, keepdims=True)

    def product(at, size):
        return sum(
            dot(part, ref[at : at + size, :], ((1,), (1,))) for part, ref in zip(scaled, weight_refs)
        )

    for at, width in ((0, 512), (512, 512), (1024, 384)):
        real = min(width, UNITS - at)
        low = product(at, real)
        high = product(UNITS + at, real)
        if real < width:
            pad = jnp.broadcast_to(squares, (32, width - real))
            low = jnp.concatenate([low, pad], axis=1)
            high = jnp.concatenate([high, pad], axis=1)
        store_shares(out_ref, low, high, at)


def hidden_body(got_ref, out_ref):
    total = jnp.sum(got_ref[...].astype(F32), axis=0)
    inv = lax.rsqrt(total[0:4, UNITS : UNITS + 1] / WIDTH + EPS)
    gate = total[0:4] * inv
    up = pltpu.roll(total, 4, 0)[0:4] * inv
    out_ref[...] = (gate / (1.0 + jnp.exp(-gate)) * up).astype(BF16)


def down_body(hidden_ref, down_ref, *refs):
    mid_refs, (out_ref, mid_ref) = refs[:4], refs[4:]
    out_ref[...] = dot(hidden_ref[:, 0:UNITS], down_ref[...]).astype(BF16)
    whose = sequences_of(lax.axis_index("y"), (128, 128), 1)
    place = chosen(whose == lax.broadcasted_iota(jnp.int32, (128, 128), 0))
    mids = jnp.concatenate([ref[...] for ref in mid_refs], axis=0)
    mid_ref[...] = dot(place, mids).astype(BF16)


def out_body(heads_ref, *refs):
    sent_refs, out_ref = refs[:4], refs[4]
    for k, ref in enumerate(sent_refs):
        out_ref[:, 128 * k : 128 * k + 128] = dot(heads_ref[...], ref[0:TOKENS_AT, :]).astype(BF16)


def moved(x, axis, shift):
    length = lax.axis_size(axis)
    return lax.ppermute(x, axis, [(i, (i + shift) % length) for i in range(length)])


def tp_parts(mine):
    pair = (mine.astype(F32) + moved(mine, "c", 1).astype(F32)).astype(BF16)
    return (pair, *(moved(pair, "x", k) for k in (1, 3, 2)))


def to_all(x, axes):
    devices = lax.axis_size(axes)
    copies = jnp.broadcast_to(x[None], (devices, *x.shape))
    got = lax.all_to_all(copies, axes, 0, 0, tiled=True)
    return got.reshape(devices * x.shape[0], x.shape[1])


def shares(x, axes):
    return lax.all_to_all(x.reshape(-1, 8, x.shape[-1]), axes, 0, 0, tiled=True)


def along_y(x):
    got = [x]
    for k in (1, 3, 2):
        got.append(moved(x, "y", k))
    return tuple(got)


def on_device(
    tokens,
    attn_gain,
    query_weight,
    key_weight,
    value_weight,
    outgate_weight,
    code_weight,
    decay_weight,
    decay_bias,
    head_gain,
    key_cache,
    value_cache,
    decay_cache,
    carried_state,
    lengths,
    output_weight,
    mlp_gain,
    gate_weight,
    up_weight,
    down_weight,
):
    seqs = key_cache.shape[0]
    read = (tokens, attn_gain[None], query_weight, key_weight, value_weight, outgate_weight, code_weight.T)
    small = (decay_weight, decay_bias[None], head_gain[None], lengths[None])
    first, sent, lifting, *small = kernel(
        project_body,
        [
            ((32 // 2, 2, 8, FIRST), BF16),
            ((SENT, 128), BF16),
            ((2 * UNITS, 128), BF16),
            *((a.shape, a.dtype) for a in small),
        ],
        [in_hbm(a) for a in (*read, mlp_gain[None])],
        (
            (output_weight, 1, 0),
            (tokens, 1, TOKENS_AT),
            (gate_weight.T, 2, 0),
            (up_weight.T, 2, UNITS),
            *((a, 3 + k, 0) for k, a in enumerate(small)),
        ),
    )
    sent = along_y(sent)
    lifting = along_y(lifting)
    caches = (decay_cache[:, :, 0], key_cache[:, :, 0], value_cache[:, :, 0], carried_state[:, 0])
    heads, new_keys, new_values = pl.pallas_call(
        attend_body,
        out_shape=(pltpu.VMEM((seqs, 256), BF16), pltpu.VMEM((seqs, 128), BF16), pltpu.VMEM((seqs, 256), BF16)),
        in_specs=[pl.BlockSpec(memory_space=pltpu.VMEM)] * 5 + [pl.BlockSpec(memory_space=pl.ANY)] * 4,
        out_specs=[pl.BlockSpec(memory_space=pltpu.VMEM)] * 3,
        scratch_shapes=[
            *(pltpu.VMEM(a.shape, a.dtype) for a in caches),
            pltpu.SemaphoreType.DMA((4,)),
        ],
        compiler_params=pltpu.CompilerParams(vmem_limit_bytes=8 << 20),
        name="attend",
    )(shares(first, KV), *small, *map(in_hbm, caches))
    (attended,) = kernel(out_body, [((32, 512), BF16)], (to_all(heads, "z"), *sent))
    middle, second = kernel(
        lift_body, [((4, 32, 128), BF16), ((4, 2, 8, SECOND), BF16)], (*tp_parts(attended), *sent, *lifting)
    )
    (hidden,) = kernel(hidden_body, [((seqs, SECOND), BF16)], (shares(second, "z"),))
    middles = (middle[0], moved(middle[2], "y", 1), moved(middle[1], "y", 3), moved(middle[3], "y", 2))
    lifted, middle = kernel(
        down_body, [((128, 128), BF16), ((128, 128), BF16)], (to_all(hidden, KV), down_weight, *middles)
    )
    mine, after, before, across = (part.astype(F32) for part in tp_parts(lifted))
    layer_out = (middle.astype(F32) + ((mine + across) + (after + before))).astype(BF16)
    return (layer_out, new_keys[:, None], new_values[:, None])


def solution(mesh):
    axes = Mesh(mesh.devices.reshape(8, 4, 4, 2), ("z", "y", "x", "c"))
    in_specs = (
        P(None, KV),
        P(KV),
        P(KV, TP),
        P(KV, TP),
        P(KV, TP),
        P(KV, TP),
        P(KV, None),
        P(None, TP),
        P(TP),
        P(),
        P(KV, None, TP, None),
        P(KV, None, TP, None),
        P(KV, None, TP, None),
        P(KV, TP, None, None),
        P(KV),
        P(TP, KV),
        P(KV),
        P(KV, TP),
        P(KV, TP),
        P(TP, KV),
    )
    out_specs = (P(None, KV), P(KV, TP, None), P(KV, TP, None))
    return jax.shard_map(
        on_device, mesh=axes, in_specs=in_specs, out_specs=out_specs, check_vma=False
    )
```

```python
import jax
import jax.numpy as jnp
from jax import lax
from jax.experimental import pallas as pl
from jax.experimental.pallas import tpu as pltpu
from jax.sharding import Mesh
from jax.sharding import PartitionSpec as P

WIDTH = 4096
EPS = 1e-06
GATE_TEMP = 16.0
KV = ("z", "y")
TP = ("x", "c")
F32 = jnp.float32
BF16 = jnp.bfloat16
FIRST = 512
CODE_AT = 256
SQUARE_AT = 272
TOKENS_AT = 256
GAIN_AT = 384
SENT = 400
UNITS = 1376
SECOND = 1408


def kernel(body, outs, args, fetched=()):
    count, more = len(args), len(fetched)

    def whole(*refs):
        arg_refs, from_refs = refs[:count], refs[count : count + more]
        out_refs = refs[count + more : -1] if more else refs[count:]
        copies = [
            pltpu.make_async_copy(
                source, out_refs[out].at[pl.ds(row, source.shape[0])], refs[-1].at[k]
            )
            for k, (source, (_, out, row)) in enumerate(zip(from_refs, fetched))
        ]
        for copy in copies:
            copy.start()
        body(*arg_refs, *out_refs)
        for copy in copies:
            copy.wait()

    return pl.pallas_call(
        whole,
        out_shape=tuple(pltpu.VMEM(*out) for out in outs),
        in_specs=[pl.BlockSpec(memory_space=pltpu.VMEM)] * count + [pl.BlockSpec(memory_space=pl.ANY)] * more,
        out_specs=[pl.BlockSpec(memory_space=pltpu.VMEM)] * len(outs),
        scratch_shapes=[pltpu.SemaphoreType.DMA((more,))] if more else [],
        compiler_params=pltpu.CompilerParams(vmem_limit_bytes=8 << 20),
    )(*args, *(in_hbm(array) for array, _, _ in fetched))


def in_hbm(x):
    return pltpu.with_memory_space_constraint(x, pltpu.HBM)


def store_shares(out_ref, low, high, at=0):
    rows, width = low.shape
    low = low.reshape(rows // 8, 8, width)
    high = high.reshape(rows // 8, 8, width)
    first = lax.broadcasted_iota(jnp.int32, low.shape, 1) < 4
    out_ref[:, 0, :, at : at + width] = jnp.where(first, low, pltpu.roll(high, 4, 1)).astype(BF16)
    out_ref[:, 1, :, at : at + width] = jnp.where(first, pltpu.roll(low, 4, 1), high).astype(BF16)


def dot(a, b, dims=((1,), (0,)), **kw):
    return lax.dot_general(a, b, (dims, ((), ())), preferred_element_type=F32, **kw)


def project_body(tok_ref, gain_ref, q_ref, k_ref, v_ref, g_ref, code_ref, mlp_gain_ref, out_ref, sent_ref, *_):
    part = mlp_gain_ref[...]
    rows = []
    for _ in range(3):
        rows.append(rounded(part))
        part = part - rows[-1]
    rows = jnp.concatenate([*rows, jnp.zeros((SENT - GAIN_AT - 3, 128), F32)], axis=0)
    sent_ref[GAIN_AT:SENT, :] = rows.astype(BF16)
    tok = tok_ref[...].astype(F32)
    scaled = (tok * gain_ref[...]).astype(BF16)
    squares = jnp.sum(tok * tok, axis=1, keepdims=True)
    code = dot(scaled, code_ref[...], ((1,), (1,)))
    lane = lax.broadcasted_iota(jnp.int32, (128, 256), 1)
    tail = jnp.concatenate([code, jnp.zeros((128, 240), F32)], axis=1)
    tail = jnp.where(lane == SQUARE_AT - CODE_AT, squares, tail)
    out_gate = dot(scaled, g_ref[...])
    head = jnp.concatenate([dot(scaled, q_ref[...]), dot(scaled, k_ref[...])], axis=1)
    store_shares(out_ref, head, out_gate)
    store_shares(out_ref, dot(scaled, v_ref[...]), tail, 256)


def rounded(x):
    return x.astype(BF16).astype(F32)


def attend_body(
    got_ref, dw_ref, bias_ref, hg_ref, len_ref, decay_hbm, key_hbm, value_hbm, state_hbm,
    heads_ref, nk_ref, nv_ref, decay_ref, key_ref, value_ref, state_ref, sems,
):
    sources = (decay_hbm, key_hbm, value_hbm, state_hbm)
    targets = (decay_ref, key_ref, value_ref, state_ref)
    copies = [pltpu.make_async_copy(a, b, sems.at[k]) for k, (a, b) in enumerate(zip(sources, targets))]
    for copy in copies:
        copy.start()
    total = jnp.sum(got_ref[...].astype(F32), axis=0)
    squares = jnp.broadcast_to(total[:, SQUARE_AT : SQUARE_AT + 1], (8, 128))
    inv_high = lax.rsqrt(squares / WIDTH + EPS)
    inv_low = pltpu.roll(inv_high, 4, 0)
    twice = lambda x: jnp.concatenate([x, x], axis=1)
    queries = rounded(total[:, 0:128] * inv_low * 128 ** (-0.5))
    keys = (total[:, 128:256] * inv_low).astype(BF16)
    values = (total[:, 256:512] * twice(inv_low)).astype(BF16)
    out_gate = pltpu.roll(rounded(total[:, 0:256] * twice(inv_high)), 4, 0)
    code = (total[:, CODE_AT : CODE_AT + 128] * inv_high).astype(BF16)[:, 0:16]
    pre = pltpu.roll(dot(code, dw_ref[...]) + bias_ref[...], 4, 0)
    log_sig = jnp.minimum(pre, 0.0) - jnp.log1p(jnp.exp(-jnp.abs(pre)))
    decayed = queries * jnp.exp(log_sig / GATE_TEMP)
    own = jnp.sum(queries * keys.astype(F32), axis=1, keepdims=True)
    row = lax.broadcasted_iota(jnp.int32, (64, 64), 0)
    col = lax.broadcasted_iota(jnp.int32, (64, 64), 1)
    later = (col > row).astype(F32)
    position = lax.broadcasted_iota(jnp.int32, (64, 128), 0)
    copies[0].wait()
    live = [position < len_ref[:, b : b + 1] for b in range(4)]
    kept = [jnp.where(live[b], decay_ref[b], 0.0) for b in range(4)]
    sums = dot(later, jnp.concatenate(kept, axis=1), precision=lax.Precision.HIGHEST)
    totals = jnp.concatenate([jnp.sum(k, axis=0, keepdims=True) for k in kept], axis=0)
    carry = decayed[0:4] * jnp.exp(totals)
    columns = jnp.concatenate([carry, carry], axis=0).T
    for copy in copies[1:]:
        copy.wait()
    mixed = []
    for b in range(4):
        keyed = key_ref[b].astype(F32) * jnp.exp(sums[:, 128 * b : 128 * b + 128])
        scores = jnp.sum(jnp.where(live[b], keyed * decayed[b : b + 1], 0.0), axis=1, keepdims=True)
        within = jnp.sum(rounded(scores) * value_ref[b].astype(F32), axis=0, keepdims=True)
        carried = jnp.sum(columns[:, b : b + 1] * state_ref[b], axis=0, keepdims=True)
        mixed.append(carried + within)
    mixed = jnp.concatenate(mixed, axis=0) + own[0:4] * values[0:4].astype(F32)
    scale = lax.rsqrt(jnp.mean(mixed * mixed, axis=1, keepdims=True) + EPS)
    gate = out_gate[0:4]
    heads_ref[...] = (mixed * scale * hg_ref[...] * (gate / (1.0 + jnp.exp(-gate)))).astype(BF16)
    nk_ref[...] = keys[0:4]
    nv_ref[...] = values[0:4]


def sequences_of(y, shape, dim):
    place = lax.broadcasted_iota(jnp.int32, shape, dim)
    group = place // 32
    owner = jnp.where(group == 0, y, jnp.where(group == 1, y + 3, jnp.where(group == 2, y + 1, y + 2))) % 4
    return (place % 32) // 4 * 16 + owner * 4 + place % 4


def chosen(condition):
    return jnp.where(condition, 1.0, 0.0).astype(BF16)


def lift_body(mine_ref, after_ref, before_ref, across_ref, *refs):
    sent_refs, weight_refs, (gate_ref, up_ref), (mid_ref, out_ref) = refs[:4], refs[4:7], refs[7:9], refs[9:]
    gate_from = [(ref, 0) for ref in weight_refs] + [(gate_ref, 0)]
    up_from = [(ref, UNITS) for ref in weight_refs] + [(up_ref, 0)]
    attended = (mine_ref[...].astype(F32) + across_ref[...].astype(F32)) + (
        after_ref[...].astype(F32) + before_ref[...].astype(F32)
    )
    own = sequences_of(lax.axis_index("y"), (32, 128), 0)
    pick = chosen(own == lax.broadcasted_iota(jnp.int32, (32, 128), 1))
    tok = jnp.concatenate([dot(pick, ref[TOKENS_AT:GAIN_AT, :]) for ref in sent_refs], axis=1)
    middle = (tok + attended).astype(BF16)
    mid = middle.astype(F32)
    scaled = []
    for k, ref in enumerate(sent_refs):
        mid_ref[k] = middle[:, 128 * k : 128 * k + 128]
        gain = jnp.sum(ref[GAIN_AT:SENT, :].astype(F32), axis=0, keepdims=True)
        scaled.append((mid[:, 128 * k : 128 * k + 128] * gain).astype(BF16))
    squares = jnp.sum(mid * mid, axis=1, keepdims=True)

    def product(weights, at, size):
        return sum(
            dot(part, ref[base + at : base + at + size, :], ((1,), (1,)))
            for part, (ref, base) in zip(scaled, weights)
        )

    for at, width in ((0, 512), (512, 512), (1024, 384)):
        real = min(width, UNITS - at)
        low = product(gate_from, at, real)
        high = product(up_from, at, real)
        if real < width:
            pad = jnp.broadcast_to(squares, (32, width - real))
            low = jnp.concatenate([low, pad], axis=1)
            high = jnp.concatenate([high, pad], axis=1)
        store_shares(out_ref, low, high, at)


def hidden_body(got_ref, out_ref):
    total = jnp.sum(got_ref[...].astype(F32), axis=0)
    inv = lax.rsqrt(total[0:4, UNITS : UNITS + 1] / WIDTH + EPS)
    gate = total[0:4] * inv
    up = pltpu.roll(total, 4, 0)[0:4] * inv
    out_ref[...] = (gate / (1.0 + jnp.exp(-gate)) * up).astype(BF16)


def down_body(hidden_ref, down_ref, *refs):
    mid_refs, (out_ref, mid_ref) = refs[:4], refs[4:]
    out_ref[...] = dot(hidden_ref[:, 0:UNITS], down_ref[...]).astype(BF16)
    whose = sequences_of(lax.axis_index("y"), (128, 128), 1)
    place = chosen(whose == lax.broadcasted_iota(jnp.int32, (128, 128), 0))
    mids = jnp.concatenate([ref[...] for ref in mid_refs], axis=0)
    mid_ref[...] = dot(place, mids).astype(BF16)


def out_body(heads_ref, *refs):
    sent_refs, out_ref = refs[:4], refs[4]
    for k, ref in enumerate(sent_refs):
        out_ref[:, 128 * k : 128 * k + 128] = dot(heads_ref[...], ref[0:TOKENS_AT, :]).astype(BF16)


def moved(x, axis, shift):
    length = lax.axis_size(axis)
    return lax.ppermute(x, axis, [(i, (i + shift) % length) for i in range(length)])


def tp_parts(mine):
    pair = (mine.astype(F32) + moved(mine, "c", 1).astype(F32)).astype(BF16)
    return (pair, *(moved(pair, "x", k) for k in (1, 3, 2)))


def to_all(x, axes):
    devices = lax.axis_size(axes)
    copies = jnp.broadcast_to(x[None], (devices, *x.shape))
    got = lax.all_to_all(copies, axes, 0, 0, tiled=True)
    return got.reshape(devices * x.shape[0], x.shape[1])


def shares(x, axes):
    return lax.all_to_all(x.reshape(-1, 8, x.shape[-1]), axes, 0, 0, tiled=True)


def layer(
    tokens,
    attn_gain,
    query_weight,
    key_weight,
    value_weight,
    outgate_weight,
    code_weight,
    decay_weight,
    decay_bias,
    head_gain,
    key_cache,
    value_cache,
    decay_cache,
    carried_state,
    lengths,
    output_weight,
    mlp_gain,
    gate_weight,
    up_weight,
    down_weight,
):
    seqs = key_cache.shape[0]
    read = (tokens, attn_gain[None], query_weight, key_weight, value_weight, outgate_weight, code_weight.T)
    small = (decay_weight, decay_bias[None], head_gain[None], lengths[None])
    first, sent, lifting, *small = kernel(
        project_body,
        [
            ((32 // 2, 2, 8, FIRST), BF16),
            ((SENT, 128), BF16),
            ((2 * UNITS, 128), BF16),
            *((a.shape, a.dtype) for a in small),
        ],
        [in_hbm(a) for a in (*read, mlp_gain[None])],
        (
            (output_weight, 1, 0),
            (tokens, 1, TOKENS_AT),
            (gate_weight.T, 2, 0),
            (up_weight.T, 2, UNITS),
            *((a, 3 + k, 0) for k, a in enumerate(small)),
        ),
    )
    sent = (sent, *(moved(sent, "y", k) for k in (1, 3, 2)))
    before, after = (moved(lifting, "y", k) for k in (1, 3))
    caches = (decay_cache[:, :, 0], key_cache[:, :, 0], value_cache[:, :, 0], carried_state[:, 0])
    heads, new_keys, new_values = pl.pallas_call(
        attend_body,
        out_shape=(pltpu.VMEM((seqs, 256), BF16), pltpu.VMEM((seqs, 128), BF16), pltpu.VMEM((seqs, 256), BF16)),
        in_specs=[pl.BlockSpec(memory_space=pltpu.VMEM)] * 5 + [pl.BlockSpec(memory_space=pl.ANY)] * 4,
        out_specs=[pl.BlockSpec(memory_space=pltpu.VMEM)] * 3,
        scratch_shapes=[
            *(pltpu.VMEM(a.shape, a.dtype) for a in caches),
            pltpu.SemaphoreType.DMA((4,)),
        ],
        compiler_params=pltpu.CompilerParams(vmem_limit_bytes=8 << 20),
        name="attend",
    )(shares(first, KV), *small, *map(in_hbm, caches))
    (attended,) = kernel(out_body, [((32, 512), BF16)], (to_all(heads, "z"), *sent))
    across = (moved(before[:UNITS], "y", 1), moved(after[UNITS:], "y", 3))
    middle, second = kernel(
        lift_body,
        [((4, 32, 128), BF16), ((4, 2, 8, SECOND), BF16)],
        (*tp_parts(attended), *sent, lifting, before, after, *across),
    )
    (hidden,) = kernel(hidden_body, [((seqs, SECOND), BF16)], (shares(second, "z"),))
    middles = (middle[0], moved(middle[2], "y", 1), moved(middle[1], "y", 3), moved(middle[3], "y", 2))
    lifted, middle = kernel(
        down_body, [((128, 128), BF16), ((128, 128), BF16)], (to_all(hidden, KV), down_weight, *middles)
    )
    mine, after, before, across = (part.astype(F32) for part in tp_parts(lifted))
    layer_out = (middle.astype(F32) + ((mine + across) + (after + before))).astype(BF16)
    return (layer_out, new_keys[:, None], new_values[:, None])


def solution(mesh):
    axes = Mesh(mesh.devices.reshape(8, 4, 4, 2), ("z", "y", "x", "c"))
    in_specs = (
        P(None, KV),
        P(KV),
        P(KV, TP),
        P(KV, TP),
        P(KV, TP),
        P(KV, TP),
        P(KV, None),
        P(None, TP),
        P(TP),
        P(),
        P(KV, None, TP, None),
        P(KV, None, TP, None),
        P(KV, None, TP, None),
        P(KV, TP, None, None),
        P(KV),
        P(TP, KV),
        P(KV),
        P(KV, TP),
        P(KV, TP),
        P(TP, KV),
    )
    out_specs = (P(None, KV), P(KV, TP, None), P(KV, TP, None))
    return jax.shard_map(layer, mesh=axes, in_specs=in_specs, out_specs=out_specs, check_vma=False)
```

```python
import jax
import jax.numpy as jnp
from jax import lax
from jax.experimental import pallas as pl
from jax.experimental.pallas import tpu as pltpu
from jax.sharding import Mesh
from jax.sharding import PartitionSpec as P

WIDTH = 4096
EPS = 1e-06
GATE_TEMP = 16.0
KV = ("z", "y")
TP = ("x", "c")
F32 = jnp.float32
BF16 = jnp.bfloat16
FIRST = 512
CODE_AT = 256
SQUARE_AT = 272
TOKENS_AT = 256
GAIN_AT = 384
SENT = 400
UNITS = 1376
SECOND = 1408


def kernel(body, outs, args, fetched=()):
    count, more = len(args), len(fetched)

    def whole(*refs):
        arg_refs, from_refs = refs[:count], refs[count : count + more]
        out_refs = refs[count + more : -1] if more else refs[count:]
        copies = [
            pltpu.make_async_copy(
                source, out_refs[out].at[pl.ds(row, source.shape[0])], refs[-1].at[k]
            )
            for k, (source, (_, out, row)) in enumerate(zip(from_refs, fetched))
        ]
        for copy in copies:
            copy.start()
        body(*arg_refs, *out_refs)
        for copy in copies:
            copy.wait()

    return pl.pallas_call(
        whole,
        out_shape=tuple(pltpu.VMEM(*out) for out in outs),
        in_specs=[pl.BlockSpec(memory_space=pltpu.VMEM)] * count + [pl.BlockSpec(memory_space=pl.ANY)] * more,
        out_specs=[pl.BlockSpec(memory_space=pltpu.VMEM)] * len(outs),
        scratch_shapes=[pltpu.SemaphoreType.DMA((more,))] if more else [],
        compiler_params=pltpu.CompilerParams(vmem_limit_bytes=8 << 20),
    )(*args, *(in_hbm(array) for array, _, _ in fetched))


def in_hbm(x):
    return pltpu.with_memory_space_constraint(x, pltpu.HBM)


def store_shares(out_ref, low, high, at=0):
    rows, width = low.shape
    low = low.reshape(rows // 8, 8, width)
    high = high.reshape(rows // 8, 8, width)
    first = lax.broadcasted_iota(jnp.int32, low.shape, 1) < 4
    out_ref[:, 0, :, at : at + width] = jnp.where(first, low, pltpu.roll(high, 4, 1)).astype(BF16)
    out_ref[:, 1, :, at : at + width] = jnp.where(first, pltpu.roll(low, 4, 1), high).astype(BF16)


def dot(a, b, dims=((1,), (0,)), **kw):
    return lax.dot_general(a, b, (dims, ((), ())), preferred_element_type=F32, **kw)


def project_body(tok_ref, gain_ref, q_ref, k_ref, v_ref, g_ref, code_ref, mlp_gain_ref, out_ref, sent_ref, *_):
    part = mlp_gain_ref[...]
    rows = []
    for _ in range(3):
        rows.append(rounded(part))
        part = part - rows[-1]
    rows = jnp.concatenate([*rows, jnp.zeros((SENT - GAIN_AT - 3, 128), F32)], axis=0)
    sent_ref[GAIN_AT:SENT, :] = rows.astype(BF16)
    tok = tok_ref[...].astype(F32)
    scaled = (tok * gain_ref[...]).astype(BF16)
    squares = jnp.sum(tok * tok, axis=1, keepdims=True)
    code = dot(scaled, code_ref[...], ((1,), (1,)))
    lane = lax.broadcasted_iota(jnp.int32, (128, 256), 1)
    tail = jnp.concatenate([code, jnp.zeros((128, 240), F32)], axis=1)
    tail = jnp.where(lane == SQUARE_AT - CODE_AT, squares, tail)
    out_gate = dot(scaled, g_ref[...])
    head = jnp.concatenate([dot(scaled, q_ref[...]), dot(scaled, k_ref[...])], axis=1)
    store_shares(out_ref, head, out_gate)
    store_shares(out_ref, dot(scaled, v_ref[...]), tail, 256)


def rounded(x):
    return x.astype(BF16).astype(F32)


def attend_body(
    got_ref, dw_ref, bias_ref, hg_ref, len_ref, decay_hbm, key_hbm, value_hbm, state_hbm,
    heads_ref, nk_ref, nv_ref, decay_ref, key_ref, value_ref, state_ref, sems,
):
    sources = (decay_hbm, key_hbm, value_hbm, state_hbm)
    targets = (decay_ref, key_ref, value_ref, state_ref)
    copies = [pltpu.make_async_copy(a, b, sems.at[k]) for k, (a, b) in enumerate(zip(sources, targets))]
    for copy in copies:
        copy.start()
    total = jnp.sum(got_ref[...].astype(F32), axis=0)
    squares = jnp.broadcast_to(total[:, SQUARE_AT : SQUARE_AT + 1], (8, 128))
    inv_high = lax.rsqrt(squares / WIDTH + EPS)
    inv_low = pltpu.roll(inv_high, 4, 0)
    twice = lambda x: jnp.concatenate([x, x], axis=1)
    queries = rounded(total[:, 0:128] * inv_low * 128 ** (-0.5))
    keys = (total[:, 128:256] * inv_low).astype(BF16)
    values = (total[:, 256:512] * twice(inv_low)).astype(BF16)
    out_gate = pltpu.roll(rounded(total[:, 0:256] * twice(inv_high)), 4, 0)
    code = (total[:, CODE_AT : CODE_AT + 128] * inv_high).astype(BF16)[:, 0:16]
    pre = pltpu.roll(dot(code, dw_ref[...]) + bias_ref[...], 4, 0)
    log_sig = jnp.minimum(pre, 0.0) - jnp.log1p(jnp.exp(-jnp.abs(pre)))
    decayed = queries * jnp.exp(log_sig / GATE_TEMP)
    own = jnp.sum(queries * keys.astype(F32), axis=1, keepdims=True)
    row = lax.broadcasted_iota(jnp.int32, (64, 64), 0)
    col = lax.broadcasted_iota(jnp.int32, (64, 64), 1)
    later = (col > row).astype(F32)
    position = lax.broadcasted_iota(jnp.int32, (64, 128), 0)
    copies[0].wait()
    live = [position < len_ref[:, b : b + 1] for b in range(4)]
    kept = [jnp.where(live[b], decay_ref[b], 0.0) for b in range(4)]
    sums = dot(later, jnp.concatenate(kept, axis=1), precision=lax.Precision.HIGHEST)
    totals = jnp.concatenate([jnp.sum(k, axis=0, keepdims=True) for k in kept], axis=0)
    carry = decayed[0:4] * jnp.exp(totals)
    columns = jnp.concatenate([carry, carry], axis=0).T
    for copy in copies[1:]:
        copy.wait()
    mixed = []
    for b in range(4):
        keyed = key_ref[b].astype(F32) * jnp.exp(sums[:, 128 * b : 128 * b + 128])
        scores = jnp.sum(jnp.where(live[b], keyed * decayed[b : b + 1], 0.0), axis=1, keepdims=True)
        within = jnp.sum(rounded(scores) * value_ref[b].astype(F32), axis=0, keepdims=True)
        carried = jnp.sum(columns[:, b : b + 1] * state_ref[b], axis=0, keepdims=True)
        mixed.append(carried + within)
    mixed = jnp.concatenate(mixed, axis=0) + own[0:4] * values[0:4].astype(F32)
    scale = lax.rsqrt(jnp.mean(mixed * mixed, axis=1, keepdims=True) + EPS)
    gate = out_gate[0:4]
    heads_ref[...] = (mixed * scale * hg_ref[...] * (gate / (1.0 + jnp.exp(-gate)))).astype(BF16)
    nk_ref[...] = keys[0:4]
    nv_ref[...] = values[0:4]


def sequences_of(y, shape, dim):
    place = lax.broadcasted_iota(jnp.int32, shape, dim)
    group = place // 32
    owner = jnp.where(group == 0, y, jnp.where(group == 1, y + 3, jnp.where(group == 2, y + 1, y + 2))) % 4
    return (place % 32) // 4 * 16 + owner * 4 + place % 4


def chosen(condition):
    return jnp.where(condition, 1.0, 0.0).astype(BF16)


def lift_body(mine_ref, after_ref, before_ref, across_ref, *refs):
    sent_refs, gate_refs, up_refs, (mid_ref, out_ref) = refs[:4], refs[4:8], refs[8:12], refs[12:]
    attended = (mine_ref[...].astype(F32) + across_ref[...].astype(F32)) + (
        after_ref[...].astype(F32) + before_ref[...].astype(F32)
    )
    own = sequences_of(lax.axis_index("y"), (32, 128), 0)
    pick = chosen(own == lax.broadcasted_iota(jnp.int32, (32, 128), 1))
    tok = jnp.concatenate([dot(pick, ref[TOKENS_AT:GAIN_AT, :]) for ref in sent_refs], axis=1)
    middle = (tok + attended).astype(BF16)
    mid = middle.astype(F32)
    scaled = []
    for k, ref in enumerate(sent_refs):
        mid_ref[k] = middle[:, 128 * k : 128 * k + 128]
        gain = jnp.sum(ref[GAIN_AT:SENT, :].astype(F32), axis=0, keepdims=True)
        scaled.append((mid[:, 128 * k : 128 * k + 128] * gain).astype(BF16))
    squares = jnp.sum(mid * mid, axis=1, keepdims=True)

    def product(weights, at, size):
        return sum(
            dot(part, ref[at : at + size, :], ((1,), (1,))) for part, ref in zip(scaled, weights)
        )

    for at, width in ((0, 512), (512, 512), (1024, 384)):
        real = min(width, UNITS - at)
        low = product(gate_refs, at, real)
        high = product(up_refs, at, real)
        if real < width:
            pad = jnp.broadcast_to(squares, (32, width - real))
            low = jnp.concatenate([low, pad], axis=1)
            high = jnp.concatenate([high, pad], axis=1)
        store_shares(out_ref, low, high, at)


def hidden_body(got_ref, out_ref):
    total = jnp.sum(got_ref[...].astype(F32), axis=0)
    inv = lax.rsqrt(total[0:4, UNITS : UNITS + 1] / WIDTH + EPS)
    gate = total[0:4] * inv
    up = pltpu.roll(total, 4, 0)[0:4] * inv
    out_ref[...] = (gate / (1.0 + jnp.exp(-gate)) * up).astype(BF16)


def down_body(hidden_ref, down_ref, *refs):
    mid_refs, (out_ref, mid_ref) = refs[:4], refs[4:]
    out_ref[...] = dot(hidden_ref[:, 0:UNITS], down_ref[...]).astype(BF16)
    whose = sequences_of(lax.axis_index("y"), (128, 128), 1)
    place = chosen(whose == lax.broadcasted_iota(jnp.int32, (128, 128), 0))
    mids = jnp.concatenate([ref[...] for ref in mid_refs], axis=0)
    mid_ref[...] = dot(place, mids).astype(BF16)


def out_body(heads_ref, *refs):
    sent_refs, out_ref = refs[:4], refs[4]
    for k, ref in enumerate(sent_refs):
        out_ref[:, 128 * k : 128 * k + 128] = dot(heads_ref[...], ref[0:TOKENS_AT, :]).astype(BF16)


def moved(x, axis, shift):
    length = lax.axis_size(axis)
    return lax.ppermute(x, axis, [(i, (i + shift) % length) for i in range(length)])


def tp_parts(mine):
    pair = (mine.astype(F32) + moved(mine, "c", 1).astype(F32)).astype(BF16)
    return (pair, *(moved(pair, "x", k) for k in (1, 3, 2)))


def to_all(x, axes):
    devices = lax.axis_size(axes)
    copies = jnp.broadcast_to(x[None], (devices, *x.shape))
    got = lax.all_to_all(copies, axes, 0, 0, tiled=True)
    return got.reshape(devices * x.shape[0], x.shape[1])


def shares(x, axes):
    return lax.all_to_all(x.reshape(-1, 8, x.shape[-1]), axes, 0, 0, tiled=True)


def layer(
    tokens,
    attn_gain,
    query_weight,
    key_weight,
    value_weight,
    outgate_weight,
    code_weight,
    decay_weight,
    decay_bias,
    head_gain,
    key_cache,
    value_cache,
    decay_cache,
    carried_state,
    lengths,
    output_weight,
    mlp_gain,
    gate_weight,
    up_weight,
    down_weight,
):
    seqs = key_cache.shape[0]
    read = (tokens, attn_gain[None], query_weight, key_weight, value_weight, outgate_weight, code_weight.T)
    small = (decay_weight, decay_bias[None], head_gain[None], lengths[None])
    gate, up = gate_weight.T, up_weight.T
    first, sent, *small = kernel(
        project_body,
        [
            ((32 // 2, 2, 8, FIRST), BF16),
            ((SENT, 128), BF16),
            *((a.shape, a.dtype) for a in small),
        ],
        [in_hbm(a) for a in (*read, mlp_gain[None])],
        (
            (output_weight, 1, 0),
            (tokens, 1, TOKENS_AT),
            *((a, 2 + k, 0) for k, a in enumerate(small)),
        ),
    )
    sent = (sent, *(moved(sent, "y", k) for k in (1, 3, 2)))
    gates = [gate, *(moved(gate, "y", k) for k in (1, 3))]
    ups = [up, *(moved(up, "y", k) for k in (1, 3))]
    caches = (decay_cache[:, :, 0], key_cache[:, :, 0], value_cache[:, :, 0], carried_state[:, 0])
    first = shares(first, KV)
    heads, new_keys, new_values = pl.pallas_call(
        attend_body,
        out_shape=(pltpu.VMEM((seqs, 256), BF16), pltpu.VMEM((seqs, 128), BF16), pltpu.VMEM((seqs, 256), BF16)),
        in_specs=[pl.BlockSpec(memory_space=pltpu.VMEM)] * 5 + [pl.BlockSpec(memory_space=pl.ANY)] * 4,
        out_specs=[pl.BlockSpec(memory_space=pltpu.VMEM)] * 3,
        scratch_shapes=[
            *(pltpu.VMEM(a.shape, a.dtype) for a in caches),
            pltpu.SemaphoreType.DMA((4,)),
        ],
        compiler_params=pltpu.CompilerParams(vmem_limit_bytes=8 << 20),
        name="attend",
    )(first, *small, *map(in_hbm, caches))
    heads = to_all(heads, "z")
    (attended,) = kernel(out_body, [((32, 512), BF16)], (heads, *sent))
    gates.append(moved(gates[1], "y", 1))
    ups.append(moved(ups[2], "y", 3))
    middle, second = kernel(
        lift_body, [((4, 32, 128), BF16), ((4, 2, 8, SECOND), BF16)], (*tp_parts(attended), *sent, *gates, *ups)
    )
    (hidden,) = kernel(hidden_body, [((seqs, SECOND), BF16)], (shares(second, "z"),))
    middles = (middle[0], moved(middle[2], "y", 1), moved(middle[1], "y", 3), moved(middle[3], "y", 2))
    lifted, middle = kernel(
        down_body, [((128, 128), BF16), ((128, 128), BF16)], (to_all(hidden, KV), down_weight, *middles)
    )
    mine, after, before, across = (part.astype(F32) for part in tp_parts(lifted))
    layer_out = (middle.astype(F32) + ((mine + across) + (after + before))).astype(BF16)
    return (layer_out, new_keys[:, None], new_values[:, None])


def solution(mesh):
    axes = Mesh(mesh.devices.reshape(8, 4, 4, 2), ("z", "y", "x", "c"))
    in_specs = (
        P(None, KV),
        P(KV),
        P(KV, TP),
        P(KV, TP),
        P(KV, TP),
        P(KV, TP),
        P(KV, None),
        P(None, TP),
        P(TP),
        P(),
        P(KV, None, TP, None),
        P(KV, None, TP, None),
        P(KV, None, TP, None),
        P(KV, TP, None, None),
        P(KV),
        P(TP, KV),
        P(KV),
        P(KV, TP),
        P(KV, TP),
        P(TP, KV),
    )
    out_specs = (P(None, KV), P(KV, TP, None), P(KV, TP, None))
    return jax.shard_map(layer, mesh=axes, in_specs=in_specs, out_specs=out_specs, check_vma=False)
```

```python
import jax
import jax.numpy as jnp
from jax import lax
from jax.experimental import pallas as pl
from jax.experimental.pallas import tpu as pltpu
from jax.sharding import Mesh
from jax.sharding import PartitionSpec as P

WIDTH = 4096
EPS = 1e-06
GATE_TEMP = 16.0
KV = ("z", "y")
TP = ("x", "c")
F32 = jnp.float32
BF16 = jnp.bfloat16
FIRST = 896
CODE_AT = 768
SQUARE_AT = 784
TOKENS_AT = 256
GAIN_AT = 384
SENT = 400
UNITS = 1376
SECOND = 1408


def kernel(body, outs, args, fetched=()):
    count, more = len(args), len(fetched)

    def whole(*refs):
        arg_refs, from_refs = refs[:count], refs[count : count + more]
        out_refs = refs[count + more : -1] if more else refs[count:]
        copies = [
            pltpu.make_async_copy(
                source, out_refs[out].at[pl.ds(row, source.shape[0])], refs[-1].at[k]
            )
            for k, (source, (_, out, row)) in enumerate(zip(from_refs, fetched))
        ]
        for copy in copies:
            copy.start()
        body(*arg_refs, *out_refs)
        for copy in copies:
            copy.wait()

    return pl.pallas_call(
        whole,
        out_shape=tuple(pltpu.VMEM(*out) for out in outs),
        in_specs=[pl.BlockSpec(memory_space=pltpu.VMEM)] * count + [pl.BlockSpec(memory_space=pl.ANY)] * more,
        out_specs=[pl.BlockSpec(memory_space=pltpu.VMEM)] * len(outs),
        scratch_shapes=[pltpu.SemaphoreType.DMA((more,))] if more else [],
        compiler_params=pltpu.CompilerParams(vmem_limit_bytes=8 << 20),
    )(*args, *(in_hbm(array) for array, _, _ in fetched))


def in_hbm(x):
    return pltpu.with_memory_space_constraint(x, pltpu.HBM)


def store_shares(out_ref, low, high, at=0):
    rows, width = low.shape
    low = low.reshape(rows // 8, 8, width)
    high = high.reshape(rows // 8, 8, width)
    first = lax.broadcasted_iota(jnp.int32, low.shape, 1) < 4
    out_ref[:, 0, :, at : at + width] = jnp.where(first, low, pltpu.roll(high, 4, 1)).astype(BF16)
    out_ref[:, 1, :, at : at + width] = jnp.where(first, pltpu.roll(low, 4, 1), high).astype(BF16)


def dot(a, b, dims=((1,), (0,)), **kw):
    return lax.dot_general(a, b, (dims, ((), ())), preferred_element_type=F32, **kw)


def project_body(tok_ref, gain_ref, q_ref, k_ref, v_ref, g_ref, code_ref, mlp_gain_ref, out_ref, sent_ref, *_):
    part = mlp_gain_ref[...]
    rows = []
    for _ in range(3):
        rows.append(rounded(part))
        part = part - rows[-1]
    rows = jnp.concatenate([*rows, jnp.zeros((SENT - GAIN_AT - 3, 128), F32)], axis=0)
    sent_ref[GAIN_AT:SENT, :] = rows.astype(BF16)
    tok = tok_ref[...].astype(F32)
    scaled = (tok * gain_ref[...]).astype(BF16)
    squares = jnp.sum(tok * tok, axis=1, keepdims=True)
    code = dot(scaled, code_ref[...], ((1,), (1,)))
    lane = lax.broadcasted_iota(jnp.int32, (128, 128), 1)
    tail = jnp.concatenate([code, jnp.zeros((128, 112), F32)], axis=1)
    tail = jnp.where(lane == SQUARE_AT - CODE_AT, squares, tail)
    products = [dot(scaled, ref[...]) for ref in (q_ref, k_ref, v_ref, g_ref)]
    every = jnp.concatenate([*products, tail], axis=1).astype(BF16)
    for share in range(32):
        out_ref[share] = every[4 * share : 4 * share + 4]


def rounded(x):
    return x.astype(BF16).astype(F32)


def attend_body(
    got_ref, dw_ref, bias_ref, hg_ref, len_ref, decay_hbm, key_hbm, value_hbm, state_hbm,
    heads_ref, nk_ref, nv_ref, decay_ref, key_ref, value_ref, state_ref, sems,
):
    sources = (decay_hbm, key_hbm, value_hbm, state_hbm)
    targets = (decay_ref, key_ref, value_ref, state_ref)
    copies = [pltpu.make_async_copy(a, b, sems.at[k]) for k, (a, b) in enumerate(zip(sources, targets))]
    for copy in copies:
        copy.start()
    total = jnp.sum(got_ref[...].astype(F32), axis=0)
    inv = lax.rsqrt(total[:, SQUARE_AT : SQUARE_AT + 1] / WIDTH + EPS)
    queries = rounded(total[:, 0:128] * inv * 128 ** (-0.5))
    keys = (total[:, 128:256] * inv).astype(BF16)
    values = (total[:, 256:512] * inv).astype(BF16)
    gate = rounded(total[:, 512:768] * inv)
    code = (total[:, CODE_AT : CODE_AT + 128] * inv).astype(BF16)[:, 0:16]
    pre = dot(code, dw_ref[...]) + bias_ref[...]
    log_sig = jnp.minimum(pre, 0.0) - jnp.log1p(jnp.exp(-jnp.abs(pre)))
    decayed = queries * jnp.exp(log_sig / GATE_TEMP)
    own = jnp.sum(queries * keys.astype(F32), axis=1, keepdims=True)
    row = lax.broadcasted_iota(jnp.int32, (64, 64), 0)
    col = lax.broadcasted_iota(jnp.int32, (64, 64), 1)
    later = (col > row).astype(F32)
    position = lax.broadcasted_iota(jnp.int32, (64, 128), 0)
    copies[0].wait()
    live = [position < len_ref[:, b : b + 1] for b in range(4)]
    kept = [jnp.where(live[b], decay_ref[b], 0.0) for b in range(4)]
    sums = dot(later, jnp.concatenate(kept, axis=1), precision=lax.Precision.HIGHEST)
    totals = jnp.concatenate([jnp.sum(k, axis=0, keepdims=True) for k in kept], axis=0)
    carry = decayed * jnp.exp(totals)
    columns = jnp.concatenate([carry, carry], axis=0).T
    for copy in copies[1:]:
        copy.wait()
    mixed = []
    for b in range(4):
        keyed = key_ref[b].astype(F32) * jnp.exp(sums[:, 128 * b : 128 * b + 128])
        scores = jnp.sum(jnp.where(live[b], keyed * decayed[b : b + 1], 0.0), axis=1, keepdims=True)
        within = jnp.sum(rounded(scores) * value_ref[b].astype(F32), axis=0, keepdims=True)
        carried = jnp.sum(columns[:, b : b + 1] * state_ref[b], axis=0, keepdims=True)
        mixed.append(carried + within)
    mixed = jnp.concatenate(mixed, axis=0) + own * values.astype(F32)
    scale = lax.rsqrt(jnp.mean(mixed * mixed, axis=1, keepdims=True) + EPS)
    heads_ref[...] = (mixed * scale * hg_ref[...] * (gate / (1.0 + jnp.exp(-gate)))).astype(BF16)
    nk_ref[...] = keys
    nv_ref[...] = values


def sequences_of(y, shape, dim):
    place = lax.broadcasted_iota(jnp.int32, shape, dim)
    group = place // 32
    owner = jnp.where(group == 0, y, jnp.where(group == 1, y + 3, jnp.where(group == 2, y + 1, y + 2))) % 4
    return (place % 32) // 4 * 16 + owner * 4 + place % 4


def chosen(condition):
    return jnp.where(condition, 1.0, 0.0).astype(BF16)


def lift_body(mine_ref, after_ref, before_ref, across_ref, *refs):
    sent_refs, gate_refs, up_refs, (mid_ref, out_ref) = refs[:4], refs[4:8], refs[8:12], refs[12:]
    attended = (mine_ref[...].astype(F32) + across_ref[...].astype(F32)) + (
        after_ref[...].astype(F32) + before_ref[...].astype(F32)
    )
    own = sequences_of(lax.axis_index("y"), (32, 128), 0)
    pick = chosen(own == lax.broadcasted_iota(jnp.int32, (32, 128), 1))
    tok = jnp.concatenate([dot(pick, ref[TOKENS_AT:GAIN_AT, :]) for ref in sent_refs], axis=1)
    middle = (tok + attended).astype(BF16)
    mid = middle.astype(F32)
    scaled = []
    for k, ref in enumerate(sent_refs):
        mid_ref[k] = middle[:, 128 * k : 128 * k + 128]
        gain = jnp.sum(ref[GAIN_AT:SENT, :].astype(F32), axis=0, keepdims=True)
        scaled.append((mid[:, 128 * k : 128 * k + 128] * gain).astype(BF16))
    scaled = [jnp.concatenate(scaled[k : k + 2], axis=1) for k in (0, 2)]
    squares = jnp.sum(mid * mid, axis=1, keepdims=True)

    def product(weights, at, size):
        pairs = [jnp.concatenate([ref[at : at + size, :] for ref in weights[k : k + 2]], axis=1) for k in (0, 2)]
        return sum(dot(part, pair, ((1,), (1,))) for part, pair in zip(scaled, pairs))

    for at, width in ((0, 512), (512, 512), (1024, 384)):
        real = min(width, UNITS - at)
        low = product(gate_refs, at, real)
        high = product(up_refs, at, real)
        if real < width:
            pad = jnp.broadcast_to(squares, (32, width - real))
            low = jnp.concatenate([low, pad], axis=1)
            high = jnp.concatenate([high, pad], axis=1)
        store_shares(out_ref, low, high, at)


def hidden_body(got_ref, out_ref):
    total = jnp.sum(got_ref[...].astype(F32), axis=0)
    inv = lax.rsqrt(total[0:4, UNITS : UNITS + 1] / WIDTH + EPS)
    gate = total[0:4] * inv
    up = pltpu.roll(total, 4, 0)[0:4] * inv
    out_ref[...] = (gate / (1.0 + jnp.exp(-gate)) * up).astype(BF16)


def down_body(hidden_ref, down_ref, *refs):
    mid_refs, (out_ref, mid_ref) = refs[:4], refs[4:]
    out_ref[...] = dot(hidden_ref[:, 0:UNITS], down_ref[...]).astype(BF16)
    whose = sequences_of(lax.axis_index("y"), (128, 128), 1)
    place = chosen(whose == lax.broadcasted_iota(jnp.int32, (128, 128), 0))
    mids = jnp.concatenate([ref[...] for ref in mid_refs], axis=0)
    mid_ref[...] = dot(place, mids).astype(BF16)


def out_body(heads_ref, *refs):
    sent_refs, out_ref = refs[:4], refs[4]
    for k, ref in enumerate(sent_refs):
        out_ref[:, 128 * k : 128 * k + 128] = dot(heads_ref[...], ref[0:TOKENS_AT, :]).astype(BF16)


def moved(x, axis, shift):
    length = lax.axis_size(axis)
    return lax.ppermute(x, axis, [(i, (i + shift) % length) for i in range(length)])


def tp_parts(mine):
    pair = (mine.astype(F32) + moved(mine, "c", 1).astype(F32)).astype(BF16)
    return (pair, *(moved(pair, "x", k) for k in (1, 3, 2)))


def to_all(x, axes):
    devices = lax.axis_size(axes)
    copies = jnp.broadcast_to(x[None], (devices, *x.shape))
    got = lax.all_to_all(copies, axes, 0, 0, tiled=True)
    return got.reshape(devices * x.shape[0], x.shape[1])


def shares(x, axes):
    return lax.all_to_all(x, axes, 0, 0, tiled=True)


def layer(
    tokens,
    attn_gain,
    query_weight,
    key_weight,
    value_weight,
    outgate_weight,
    code_weight,
    decay_weight,
    decay_bias,
    head_gain,
    key_cache,
    value_cache,
    decay_cache,
    carried_state,
    lengths,
    output_weight,
    mlp_gain,
    gate_weight,
    up_weight,
    down_weight,
):
    seqs = key_cache.shape[0]
    read = (tokens, attn_gain[None], query_weight, key_weight, value_weight, outgate_weight, code_weight.T)
    small = (decay_weight, decay_bias[None], head_gain[None], lengths[None])
    gate, up = gate_weight.T, up_weight.T
    first, sent, *small = kernel(
        project_body,
        [
            ((32, 4, FIRST), BF16),
            ((SENT, 128), BF16),
            *((a.shape, a.dtype) for a in small),
        ],
        [in_hbm(a) for a in (*read, mlp_gain[None])],
        (
            (output_weight, 1, 0),
            (tokens, 1, TOKENS_AT),
            *((a, 2 + k, 0) for k, a in enumerate(small)),
        ),
    )
    sent = (sent, *(moved(sent, "y", k) for k in (1, 3, 2)))
    gates = [gate, *(moved(gate, "y", k) for k in (1, 3))]
    ups = [up, *(moved(up, "y", k) for k in (1, 3))]
    caches = (decay_cache[:, :, 0], key_cache[:, :, 0], value_cache[:, :, 0], carried_state[:, 0])
    first = shares(first, KV)
    heads, new_keys, new_values = pl.pallas_call(
        attend_body,
        out_shape=(pltpu.VMEM((seqs, 256), BF16), pltpu.VMEM((seqs, 128), BF16), pltpu.VMEM((seqs, 256), BF16)),
        in_specs=[pl.BlockSpec(memory_space=pltpu.VMEM)] * 5 + [pl.BlockSpec(memory_space=pl.ANY)] * 4,
        out_specs=[pl.BlockSpec(memory_space=pltpu.VMEM)] * 3,
        scratch_shapes=[
            *(pltpu.VMEM(a.shape, a.dtype) for a in caches),
            pltpu.SemaphoreType.DMA((4,)),
        ],
        compiler_params=pltpu.CompilerParams(vmem_limit_bytes=8 << 20),
        name="attend",
    )(first, *small, *map(in_hbm, caches))
    heads = to_all(heads, "z")
    (attended,) = kernel(out_body, [((32, 512), BF16)], (heads, *sent))
    gates.append(moved(gates[1], "y", 1))
    ups.append(moved(ups[2], "y", 3))
    middle, second = kernel(
        lift_body, [((4, 32, 128), BF16), ((4, 2, 8, SECOND), BF16)], (*tp_parts(attended), *sent, *gates, *ups)
    )
    (hidden,) = kernel(hidden_body, [((seqs, SECOND), BF16)], (shares(second.reshape(8, 8, SECOND), "z"),))
    middles = (middle[0], moved(middle[2], "y", 1), moved(middle[1], "y", 3), moved(middle[3], "y", 2))
    lifted, middle = kernel(
        down_body, [((128, 128), BF16), ((128, 128), BF16)], (to_all(hidden, KV), down_weight, *middles)
    )
    mine, after, before, across = (part.astype(F32) for part in tp_parts(lifted))
    layer_out = (middle.astype(F32) + ((mine + across) + (after + before))).astype(BF16)
    return (layer_out, new_keys[:, None], new_values[:, None])


def solution(mesh):
    axes = Mesh(mesh.devices.reshape(8, 4, 4, 2), ("z", "y", "x", "c"))
    in_specs = (
        P(None, KV),
        P(KV),
        P(KV, TP),
        P(KV, TP),
        P(KV, TP),
        P(KV, TP),
        P(KV, None),
        P(None, TP),
        P(TP),
        P(),
        P(KV, None, TP, None),
        P(KV, None, TP, None),
        P(KV, None, TP, None),
        P(KV, TP, None, None),
        P(KV),
        P(TP, KV),
        P(KV),
        P(KV, TP),
        P(KV, TP),
        P(TP, KV),
    )
    out_specs = (P(None, KV), P(KV, TP, None), P(KV, TP, None))
    return jax.shard_map(layer, mesh=axes, in_specs=in_specs, out_specs=out_specs, check_vma=False)
```

```python
import jax
import jax.numpy as jnp
from jax import lax
from jax.experimental import pallas as pl
from jax.experimental.pallas import tpu as pltpu
from jax.sharding import Mesh
from jax.sharding import PartitionSpec as P

WIDTH = 4096
EPS = 1e-06
GATE_TEMP = 16.0
KV = ("z", "y")
TP = ("x", "c")
F32 = jnp.float32
BF16 = jnp.bfloat16
FIRST = 896
CODE_AT = 768
SQUARE_AT = 784
TOKENS_AT = 256
GAIN_AT = 384
SENT = 400
UNITS = 1376
SECOND = 1408


def kernel(body, outs, args, fetched=()):
    count, more = len(args), len(fetched)

    def whole(*refs):
        arg_refs, from_refs = refs[:count], refs[count : count + more]
        out_refs = refs[count + more : -1] if more else refs[count:]
        copies = [
            pltpu.make_async_copy(
                source, out_refs[out].at[pl.ds(row, source.shape[0])], refs[-1].at[k]
            )
            for k, (source, (_, out, row)) in enumerate(zip(from_refs, fetched))
        ]
        for copy in copies:
            copy.start()
        body(*arg_refs, *out_refs)
        for copy in copies:
            copy.wait()

    return pl.pallas_call(
        whole,
        out_shape=tuple(pltpu.VMEM(*out) for out in outs),
        in_specs=[pl.BlockSpec(memory_space=pltpu.VMEM)] * count + [pl.BlockSpec(memory_space=pl.ANY)] * more,
        out_specs=[pl.BlockSpec(memory_space=pltpu.VMEM)] * len(outs),
        scratch_shapes=[pltpu.SemaphoreType.DMA((more,))] if more else [],
        compiler_params=pltpu.CompilerParams(vmem_limit_bytes=8 << 20),
    )(*args, *(in_hbm(array) for array, _, _ in fetched))


def in_hbm(x):
    return pltpu.with_memory_space_constraint(x, pltpu.HBM)


def store_shares(out_ref, low, high, at=0):
    rows, width = low.shape
    low = low.reshape(rows // 8, 8, width)
    high = high.reshape(rows // 8, 8, width)
    first = lax.broadcasted_iota(jnp.int32, low.shape, 1) < 4
    out_ref[:, 0, :, at : at + width] = jnp.where(first, low, pltpu.roll(high, 4, 1)).astype(BF16)
    out_ref[:, 1, :, at : at + width] = jnp.where(first, pltpu.roll(low, 4, 1), high).astype(BF16)


def dot(a, b, dims=((1,), (0,)), **kw):
    return lax.dot_general(a, b, (dims, ((), ())), preferred_element_type=F32, **kw)


def project_body(tok_ref, gain_ref, q_ref, k_ref, v_ref, g_ref, code_ref, mlp_gain_ref, out_ref, sent_ref, *_):
    part = mlp_gain_ref[...]
    rows = []
    for _ in range(3):
        rows.append(rounded(part))
        part = part - rows[-1]
    rows = jnp.concatenate([*rows, jnp.zeros((SENT - GAIN_AT - 3, 128), F32)], axis=0)
    sent_ref[GAIN_AT:SENT, :] = rows.astype(BF16)
    tok = tok_ref[...].astype(F32)
    scaled = (tok * gain_ref[...]).astype(BF16)
    squares = jnp.sum(tok * tok, axis=1, keepdims=True)
    code = dot(scaled, code_ref[...], ((1,), (1,)))
    lane = lax.broadcasted_iota(jnp.int32, (128, 128), 1)
    tail = jnp.concatenate([code, jnp.zeros((128, 112), F32)], axis=1)
    tail = jnp.where(lane == SQUARE_AT - CODE_AT, squares, tail)
    products = [dot(scaled, ref[...]) for ref in (q_ref, k_ref, v_ref, g_ref)]
    every = jnp.concatenate([*products, tail], axis=1).astype(BF16)
    for share in range(32):
        out_ref[share] = every[4 * share : 4 * share + 4]


def rounded(x):
    return x.astype(BF16).astype(F32)


def attend_body(
    got_ref, dw_ref, bias_ref, hg_ref, len_ref, decay_hbm, key_hbm, value_hbm, state_hbm,
    heads_ref, nk_ref, nv_ref, decay_ref, key_ref, value_ref, state_ref, sems,
):
    sources = (decay_hbm, key_hbm, value_hbm, state_hbm)
    targets = (decay_ref, key_ref, value_ref, state_ref)
    copies = [pltpu.make_async_copy(a, b, sems.at[k]) for k, (a, b) in enumerate(zip(sources, targets))]
    for copy in copies:
        copy.start()
    total = jnp.sum(got_ref[...].astype(F32), axis=0)
    inv = lax.rsqrt(total[:, SQUARE_AT : SQUARE_AT + 1] / WIDTH + EPS)
    queries = rounded(total[:, 0:128] * inv * 128 ** (-0.5))
    keys = (total[:, 128:256] * inv).astype(BF16)
    values = (total[:, 256:512] * inv).astype(BF16)
    gate = rounded(total[:, 512:768] * inv)
    code = (total[:, CODE_AT : CODE_AT + 128] * inv).astype(BF16)[:, 0:16]
    pre = dot(code, dw_ref[...]) + bias_ref[...]
    log_sig = jnp.minimum(pre, 0.0) - jnp.log1p(jnp.exp(-jnp.abs(pre)))
    decayed = queries * jnp.exp(log_sig / GATE_TEMP)
    own = jnp.sum(queries * keys.astype(F32), axis=1, keepdims=True)
    row = lax.broadcasted_iota(jnp.int32, (64, 64), 0)
    col = lax.broadcasted_iota(jnp.int32, (64, 64), 1)
    later = (col > row).astype(F32)
    position = lax.broadcasted_iota(jnp.int32, (64, 128), 0)
    copies[0].wait()
    live = [position < len_ref[:, b : b + 1] for b in range(4)]
    kept = [jnp.where(live[b], decay_ref[b], 0.0) for b in range(4)]
    sums = dot(later, jnp.concatenate(kept, axis=1), precision=lax.Precision.HIGHEST)
    totals = jnp.concatenate([jnp.sum(k, axis=0, keepdims=True) for k in kept], axis=0)
    carry = decayed * jnp.exp(totals)
    columns = jnp.concatenate([carry, carry], axis=0).T
    for copy in copies[1:]:
        copy.wait()
    mixed = []
    for b in range(4):
        keyed = key_ref[b].astype(F32) * jnp.exp(sums[:, 128 * b : 128 * b + 128])
        scores = jnp.sum(jnp.where(live[b], keyed * decayed[b : b + 1], 0.0), axis=1, keepdims=True)
        within = jnp.sum(rounded(scores) * value_ref[b].astype(F32), axis=0, keepdims=True)
        carried = jnp.sum(columns[:, b : b + 1] * state_ref[b], axis=0, keepdims=True)
        mixed.append(carried + within)
    mixed = jnp.concatenate(mixed, axis=0) + own * values.astype(F32)
    scale = lax.rsqrt(jnp.mean(mixed * mixed, axis=1, keepdims=True) + EPS)
    heads_ref[...] = (mixed * scale * hg_ref[...] * (gate / (1.0 + jnp.exp(-gate)))).astype(BF16)
    nk_ref[...] = keys
    nv_ref[...] = values


def sequences_of(y, shape, dim):
    place = lax.broadcasted_iota(jnp.int32, shape, dim)
    group = place // 32
    owner = jnp.where(group == 0, y, jnp.where(group == 1, y + 3, jnp.where(group == 2, y + 1, y + 2))) % 4
    return (place % 32) // 4 * 16 + owner * 4 + place % 4


def chosen(condition):
    return jnp.where(condition, 1.0, 0.0).astype(BF16)


def lift_body(mine_ref, after_ref, before_ref, across_ref, *refs):
    sent_refs, gate_refs, up_refs, (mid_ref, out_ref) = refs[:4], refs[4:8], refs[8:12], refs[12:]
    attended = (mine_ref[...].astype(F32) + across_ref[...].astype(F32)) + (
        after_ref[...].astype(F32) + before_ref[...].astype(F32)
    )
    own = sequences_of(lax.axis_index("y"), (32, 128), 0)
    pick = chosen(own == lax.broadcasted_iota(jnp.int32, (32, 128), 1))
    tok = jnp.concatenate([dot(pick, ref[TOKENS_AT:GAIN_AT, :]) for ref in sent_refs], axis=1)
    middle = (tok + attended).astype(BF16)
    mid = middle.astype(F32)
    scaled = []
    for k, ref in enumerate(sent_refs):
        mid_ref[k] = middle[:, 128 * k : 128 * k + 128]
        gain = jnp.sum(ref[GAIN_AT:SENT, :].astype(F32), axis=0, keepdims=True)
        scaled.append((mid[:, 128 * k : 128 * k + 128] * gain).astype(BF16))
    scaled = [jnp.concatenate(scaled[k : k + 2], axis=1) for k in (0, 2)]
    squares = jnp.sum(mid * mid, axis=1, keepdims=True)

    def product(weights, at, size):
        pairs = [jnp.concatenate([ref[at : at + size, :] for ref in weights[k : k + 2]], axis=1) for k in (0, 2)]
        return sum(dot(part, pair, ((1,), (1,))) for part, pair in zip(scaled, pairs))

    for at, width in ((0, 512), (512, 512), (1024, 384)):
        real = min(width, UNITS - at)
        low = product(gate_refs, at, real)
        high = product(up_refs, at, real)
        if real < width:
            pad = jnp.broadcast_to(squares, (32, width - real))
            low = jnp.concatenate([low, pad], axis=1)
            high = jnp.concatenate([high, pad], axis=1)
        store_shares(out_ref, low, high, at)


def hidden_body(got_ref, out_ref, one_ref, sems):
    total = jnp.sum(got_ref[...].astype(F32), axis=0)
    inv = lax.rsqrt(total[0:4, UNITS : UNITS + 1] / WIDTH + EPS)
    gate = total[0:4] * inv
    up = pltpu.roll(total, 4, 0)[0:4] * inv
    one_ref[...] = (gate / (1.0 + jnp.exp(-gate)) * up).astype(BF16)
    copies = [pltpu.make_async_copy(one_ref, out_ref.at[k], sems.at[k]) for k in range(32)]
    for copy in copies:
        copy.start()
    for copy in copies:
        copy.wait()


def down_body(hidden_ref, down_ref, *refs):
    mid_refs, (out_ref, mid_ref) = refs[:4], refs[4:]
    out_ref[...] = dot(hidden_ref[:, 0:UNITS], down_ref[...]).astype(BF16)
    whose = sequences_of(lax.axis_index("y"), (128, 128), 1)
    place = chosen(whose == lax.broadcasted_iota(jnp.int32, (128, 128), 0))
    mids = jnp.concatenate([ref[...] for ref in mid_refs], axis=0)
    mid_ref[...] = dot(place, mids).astype(BF16)


def out_body(heads_ref, *refs):
    sent_refs, out_ref = refs[:4], refs[4]
    for k, ref in enumerate(sent_refs):
        out_ref[:, 128 * k : 128 * k + 128] = dot(heads_ref[...], ref[0:TOKENS_AT, :]).astype(BF16)


def moved(x, axis, shift):
    length = lax.axis_size(axis)
    return lax.ppermute(x, axis, [(i, (i + shift) % length) for i in range(length)])


def tp_parts(mine):
    pair = (mine.astype(F32) + moved(mine, "c", 1).astype(F32)).astype(BF16)
    return (pair, *(moved(pair, "x", k) for k in (1, 3, 2)))


def to_all(x, axes):
    devices = lax.axis_size(axes)
    copies = jnp.broadcast_to(x[None], (devices, *x.shape))
    got = lax.all_to_all(copies, axes, 0, 0, tiled=True)
    return got.reshape(devices * x.shape[0], x.shape[1])


def shares(x, axes):
    return lax.all_to_all(x, axes, 0, 0, tiled=True)


def layer(
    tokens,
    attn_gain,
    query_weight,
    key_weight,
    value_weight,
    outgate_weight,
    code_weight,
    decay_weight,
    decay_bias,
    head_gain,
    key_cache,
    value_cache,
    decay_cache,
    carried_state,
    lengths,
    output_weight,
    mlp_gain,
    gate_weight,
    up_weight,
    down_weight,
):
    seqs = key_cache.shape[0]
    read = (tokens, attn_gain[None], query_weight, key_weight, value_weight, outgate_weight, code_weight.T)
    small = (decay_weight, decay_bias[None], head_gain[None], lengths[None])
    gate, up = gate_weight.T, up_weight.T
    first, sent, *small = kernel(
        project_body,
        [
            ((32, 4, FIRST), BF16),
            ((SENT, 128), BF16),
            *((a.shape, a.dtype) for a in small),
        ],
        [in_hbm(a) for a in (*read, mlp_gain[None])],
        (
            (output_weight, 1, 0),
            (tokens, 1, TOKENS_AT),
            *((a, 2 + k, 0) for k, a in enumerate(small)),
        ),
    )
    sent = (sent, *(moved(sent, "y", k) for k in (1, 3, 2)))
    gates = [gate, *(moved(gate, "y", k) for k in (1, 3))]
    ups = [up, *(moved(up, "y", k) for k in (1, 3))]
    caches = (decay_cache[:, :, 0], key_cache[:, :, 0], value_cache[:, :, 0], carried_state[:, 0])
    first = shares(first, KV)
    heads, new_keys, new_values = pl.pallas_call(
        attend_body,
        out_shape=(pltpu.VMEM((seqs, 256), BF16), pltpu.VMEM((seqs, 128), BF16), pltpu.VMEM((seqs, 256), BF16)),
        in_specs=[pl.BlockSpec(memory_space=pltpu.VMEM)] * 5 + [pl.BlockSpec(memory_space=pl.ANY)] * 4,
        out_specs=[pl.BlockSpec(memory_space=pltpu.VMEM)] * 3,
        scratch_shapes=[
            *(pltpu.VMEM(a.shape, a.dtype) for a in caches),
            pltpu.SemaphoreType.DMA((4,)),
        ],
        compiler_params=pltpu.CompilerParams(vmem_limit_bytes=8 << 20),
        name="attend",
    )(first, *small, *map(in_hbm, caches))
    heads = to_all(heads, "z")
    (attended,) = kernel(out_body, [((32, 512), BF16)], (heads, *sent))
    gates.append(moved(gates[1], "y", 1))
    ups.append(moved(ups[2], "y", 3))
    middle, second = kernel(
        lift_body, [((4, 32, 128), BF16), ((4, 2, 8, SECOND), BF16)], (*tp_parts(attended), *sent, *gates, *ups)
    )
    hidden = pl.pallas_call(
        hidden_body,
        out_shape=jax.ShapeDtypeStruct((32, seqs, SECOND), BF16),
        in_specs=[pl.BlockSpec(memory_space=pltpu.VMEM)],
        out_specs=pl.BlockSpec(memory_space=pl.ANY),
        scratch_shapes=[pltpu.VMEM((seqs, SECOND), BF16), pltpu.SemaphoreType.DMA((32,))],
        compiler_params=pltpu.CompilerParams(vmem_limit_bytes=8 << 20),
        name="hidden",
    )(shares(second.reshape(8, 8, SECOND), "z"))
    hidden = shares(hidden, KV).reshape(32 * seqs, SECOND)
    middles = (middle[0], moved(middle[2], "y", 1), moved(middle[1], "y", 3), moved(middle[3], "y", 2))
    lifted, middle = kernel(down_body, [((128, 128), BF16), ((128, 128), BF16)], (hidden, down_weight, *middles))
    mine, after, before, across = (part.astype(F32) for part in tp_parts(lifted))
    layer_out = (middle.astype(F32) + ((mine + across) + (after + before))).astype(BF16)
    return (layer_out, new_keys[:, None], new_values[:, None])


def solution(mesh):
    axes = Mesh(mesh.devices.reshape(8, 4, 4, 2), ("z", "y", "x", "c"))
    in_specs = (
        P(None, KV),
        P(KV),
        P(KV, TP),
        P(KV, TP),
        P(KV, TP),
        P(KV, TP),
        P(KV, None),
        P(None, TP),
        P(TP),
        P(),
        P(KV, None, TP, None),
        P(KV, None, TP, None),
        P(KV, None, TP, None),
        P(KV, TP, None, None),
        P(KV),
        P(TP, KV),
        P(KV),
        P(KV, TP),
        P(KV, TP),
        P(TP, KV),
    )
    out_specs = (P(None, KV), P(KV, TP, None), P(KV, TP, None))
    return jax.shard_map(layer, mesh=axes, in_specs=in_specs, out_specs=out_specs, check_vma=False)
```
